512 devices in a mesh: ep: 128 (over z, x, core), tp: 4 (over y).
Axes of the slice: x: 4, y: 4, z: 16, core: 2. Of those that a mesh axis runs over, the one named last changes fastest.
Arguments:
- tokens: bfloat16 [16384, 4096], P('ep', 'tp'), may hold values from -16 to 16
- expert_ids: int32 [16384, 2], P('ep'), may hold values from 0 to 127, as said below
- group_weight: float32 [16384], P('ep'), may hold values from 0.25 to 1
- expert_weight: float32 [16384, 2], P('ep'), may hold values from 0.1 to 1
- w_gate: bfloat16 [128, 4096, 512], P('ep', None, 'tp'), may hold values from -0.09375 to 0.09375
- w_up: bfloat16 [128, 4096, 512], P('ep', None, 'tp'), may hold values from -0.09375 to 0.09375
- w_down: bfloat16 [128, 512, 4096], P('ep', None, 'tp'), may hold values from -0.5 to 0.5
- norm_gain: float32 [4096], P('tp'), may hold values from 0.1 to 1.9
- norm_bias: float32 [4096], P('tp'), may hold values from -3 to 3
Outputs:
- normed: bfloat16 [16384, 4096], P('ep', 'tp')
The draws below stay inside these ranges and needn't reach their ends.
Inputs may be any that keep to these rules, and one draw needn't show every extreme that they name: `expert_ids`: each row names 2 different experts of one group, a group being 32 consecutive ids; in the rows of one ep index each group is named by a 4-th of the rows. In the rows of one ep index no expert is named more than 3 times, and in every group one expert is named exactly 3 times in the rows of every ep index.
All inputs are finite; a program needn't handle non-finite values.
Results may differ from the reference program's by a relative error of at most 0.0045.
Values may be sent and summed in bfloat16 or wider, within the bound.
No kernel may reach another device: no remote copies, remote signals or barrier semaphores. Data moves between devices by JAX's collectives and lax.ppermute only.
A program may use at most 64 MiB of HBM per device.

```python
import math
import jax
import jax.numpy as jnp
from jax import lax

D = 4096
FF = 512
GROUPS = 4
TOP_K = 2
TOK_DEV = 128
EXPERTS = 128
CAP = 3
TOKENS = 16384
N_EP = 128


def draw_tokens(key, part):
    quarter = (jnp.arange(D, dtype=jnp.int32) // (D // 4)).astype(jnp.float32)
    column_scale = 0.5 + 0.5 * quarter
    column_shift = 0.6 * (quarter - 1.5)
    values = jax.random.normal(jax.random.fold_in(key, 5), (TOKENS, D), jnp.float32)
    values = jnp.clip(values * column_scale[None, :] + column_shift[None, :], -16.0, 16.0)
    return values.astype(jnp.bfloat16)


def draw_expert_ids(key, part):
    per_group = EXPERTS // GROUPS
    pair_count = TOK_DEV // GROUPS
    block_count = TOKENS // TOK_DEV
    fixed_local = jax.random.randint(jax.random.fold_in(key, 1), (GROUPS,), 0, per_group)
    local_ids = jnp.arange(per_group, dtype=jnp.int32)
    pair_index = jnp.arange(pair_count, dtype=jnp.int32)
    first_rank = pair_index // CAP
    second_rank = (pair_index + pair_count) // CAP

    def one_block(index):
        block_key = jax.random.fold_in(key, index + 7)
        scores = jax.random.randint(jax.random.fold_in(block_key, 0), (GROUPS, per_group), 0, 1 << 20)
        scores = scores * per_group + local_ids[None, :]
        scores = jnp.where(local_ids[None, :] == fixed_local[:, None], -1, scores)
        order = jnp.argsort(scores, axis=1, stable=True).astype(jnp.int32)
        first = order[:, first_rank]
        second = order[:, second_rank]
        local_pair = jnp.stack([first, second], axis=-1)
        global_pair = local_pair + (jnp.arange(GROUPS, dtype=jnp.int32) * per_group)[:, None, None]
        flat_pairs = global_pair.reshape(TOK_DEV, 2)
        shuffle = jax.random.permutation(jax.random.fold_in(block_key, 1), TOK_DEV)
        return flat_pairs[shuffle]
    drawn = jax.vmap(one_block)(jnp.arange(block_count, dtype=jnp.int32))
    return drawn.reshape(TOKENS, 2).astype(jnp.int32)


def level_of(rng, extent, pieces, low, largest):
    factor_of, own = 1.0, jax.random.fold_in(rng, 6)
    for dim, shards_of in pieces:
        draws = jnp.exp(jax.random.uniform(jax.random.fold_in(own, dim), (shards_of,), jnp.float32, low / len(pieces), largest / len(pieces)))
        factor_of = factor_of * jnp.repeat(draws, extent[dim] // shards_of).reshape([-1 if axis == dim else 1 for axis in range(len(extent))])
    return factor_of


def noise(stream_key, shape, scale, reach, split=(), kind=jnp.bfloat16):
    gain = level_of(stream_key, shape, split, -0.22, 0.18) if split else 1.0
    values = jax.random.normal(stream_key, shape, jnp.float32) * scale * gain
    return jnp.minimum(jnp.maximum(values, -reach), reach).astype(kind)


def setup_inputs(seed: int = 0) -> dict:
    key_of = jax.random.split(jax.random.key(seed), 10)
    return {
        "tokens": draw_tokens(jax.random.fold_in(key_of[9], 71), 0),
        "expert_ids": draw_expert_ids(jax.random.fold_in(key_of[9], 71), 0),
        "group_weight": jnp.clip(jnp.exp(math.log(1.0) - 1.3862944 * jax.random.uniform(key_of[2], (TOKENS,), jnp.float32) ** level_of(key_of[2], (TOKENS,), ((0, 128),), -0.2, 0.2)), 0.25, 1.0),
        "expert_weight": jnp.clip(jnp.exp(math.log(1.0) - 2.3025851 * jax.random.uniform(key_of[3], (TOKENS, TOP_K), jnp.float32) ** level_of(key_of[3], (TOKENS, TOP_K), ((0, 128),), -0.2, 0.2)), 0.1, 1.0),
        "w_gate": noise(key_of[4], (EXPERTS, D, FF), D ** -0.5, 0.09375, ((0, 128), (2, 4))),
        "w_up": noise(key_of[5], (EXPERTS, D, FF), D ** -0.5, 0.09375, ((0, 128), (2, 4))),
        "w_down": noise(key_of[6], (EXPERTS, FF, D), (FF // 4) ** -0.5, 0.5, ((0, 128), (2, 4))),
        "norm_gain": jnp.clip(1.0 + 0.18 * jax.random.normal(key_of[7], (D,), jnp.float32), 0.1, 1.9),
        "norm_bias": noise(key_of[8], (D,), 0.5, 3.0, ((0, 4),), jnp.float32),
    }


residual_scale = 2.0 ** 0.5
norm_eps = 1e-05

def reference(tokens, expert_ids, group_weight, expert_weight, w_gate, w_up, w_down, norm_gain, norm_bias):
    block_count = TOKENS // TOK_DEV
    rows_per = N_EP * CAP
    flat_ids = expert_ids.reshape(block_count, TOK_DEV * TOP_K).astype(jnp.int32)
    one_hot = (flat_ids[:, :, None] == jnp.arange(EXPERTS, dtype=jnp.int32)[None, None, :]).astype(jnp.int32)
    prior_counts = jnp.cumsum(one_hot, axis=1) - one_hot
    slot_index = lax.optimization_barrier(jnp.sum(prior_counts * one_hot, axis=2)).astype(jnp.int32)
    block_start = (jnp.arange(block_count, dtype=jnp.int32) * CAP)[:, None]
    position = (flat_ids * rows_per + block_start + slot_index).reshape(-1).astype(jnp.int32)
    owner_token = (jnp.arange(TOKENS * TOP_K, dtype=jnp.int32) // TOP_K).astype(jnp.int32)
    slot_table = jnp.full((EXPERTS * rows_per,), TOKENS, jnp.int32).at[position].set(owner_token)
    padded = jnp.concatenate([tokens, jnp.zeros((1, D), tokens.dtype)], axis=0)

    def expert(inputs):
        table_rows, gate_w, up_w, down_w = inputs
        row_block = padded[table_rows]
        gate_sum = jnp.dot(row_block, gate_w, preferred_element_type=jnp.float32)
        up_sum = jnp.dot(row_block, up_w, preferred_element_type=jnp.float32)
        hidden = (jax.nn.silu(gate_sum) * up_sum).astype(jnp.bfloat16)
        return jnp.dot(hidden, down_w, preferred_element_type=jnp.float32).astype(jnp.bfloat16)
    results = lax.map(expert, (slot_table.reshape(EXPERTS, rows_per), w_gate, w_up, w_down))
    picked = results.reshape(EXPERTS * rows_per, D)[position].reshape(TOKENS, TOP_K, D).astype(jnp.float32)
    share_weight = group_weight[:, None] * expert_weight / lax.optimization_barrier(jnp.sum(expert_weight, axis=1, keepdims=True))
    routed = jnp.einsum('tk,tkd->td', share_weight.astype(jnp.float32), picked)
    mixed = residual_scale * tokens.astype(jnp.float32) + routed
    center = lax.optimization_barrier(jnp.mean(mixed, axis=1, keepdims=True))
    centered = mixed - center
    spread = lax.optimization_barrier(jnp.mean(centered * centered, axis=1, keepdims=True))
    normed = centered * lax.rsqrt(spread + norm_eps) * norm_gain[None, :] + norm_bias[None, :]
    return normed.astype(jnp.bfloat16)
```

```python
import jax
import jax.numpy as jnp
from jax import lax
from jax.sharding import Mesh
from jax.sharding import PartitionSpec as P

D = 4096
GROUPS = 4
TOP_K = 2
EP = ("ep_0", "ep_1", "ep_2")
LANES = 128


residual_scale = 2.0**0.5
norm_eps = 1e-05


def exchanged(tiles, axis):
    return lax.all_to_all(tiles, axis, 0, 0, tiled=True)


def permuted(tiles, axis):
    peers = lax.axis_size(axis)
    own = lax.axis_index(axis)
    result = [lax.dynamic_index_in_dim(tiles, own, 0, keepdims=False)]
    for turn in range(1, peers):
        block = lax.dynamic_index_in_dim(tiles, (own + turn) % peers, 0, keepdims=False)
        moves = [(i, (i + turn) % peers) for i in range(peers)]
        result.append(lax.ppermute(block, axis, moves))
    return result


def from_everyone(value, axis):
    peers = lax.axis_size(axis)
    return exchanged(jnp.broadcast_to(value[None], (peers, *value.shape)), axis)


def on_device(
    tokens, expert_ids, group_weight, expert_weight, w_gate, w_up, w_down, norm_gain, norm_bias
):
    tok_count, width = tokens.shape
    expert_count = lax.axis_size(EP)
    peers = lax.axis_size("tp")
    hid = w_gate.shape[2]
    capacity = min(tok_count // GROUPS, 3 * TOP_K * tok_count // (2 * expert_count))
    rows = expert_count * capacity
    pair_count = tok_count * TOP_K
    gate_up = jnp.concatenate(
        [w_gate.reshape(peers, width, hid), w_up.reshape(peers, width, hid)], axis=1
    )
    gate_up = permuted(gate_up, "tp")

    flat_ids = expert_ids.reshape(pair_count)
    one_hot = (flat_ids[:, None] == jnp.arange(expert_count, dtype=jnp.int32)[None, :]).astype(
        jnp.float32
    )
    earlier = (jnp.arange(pair_count)[:, None] > jnp.arange(pair_count)[None, :]).astype(
        jnp.float32
    )
    prior_counts = jnp.dot(
        earlier, one_hot, preferred_element_type=jnp.float32, precision=lax.Precision.HIGHEST
    )
    slot_index = jnp.sum(prior_counts * one_hot, axis=1).astype(jnp.int32)
    position = flat_ids * capacity + slot_index
    position_of = position.reshape(tok_count, TOP_K)
    slots = jnp.arange(rows, dtype=jnp.int32)
    select = (
        (slots[:, None] == position_of[None, :, 0]) | (slots[:, None] == position_of[None, :, 1])
    ).astype(jnp.bfloat16)
    outgoing = jnp.dot(select, tokens, preferred_element_type=jnp.float32).astype(jnp.bfloat16)
    tiles = outgoing.reshape(expert_count, capacity * width // LANES, LANES)
    row_block = exchanged(tiles, EP).reshape(rows, width)

    own = lax.axis_index("tp")
    partial = [
        jnp.einsum(
            "rk,gkn->rgn",
            row_block,
            block.reshape(2, width, hid),
            preferred_element_type=jnp.float32,
        )
        .astype(jnp.bfloat16)
        .reshape(rows, 2 * hid)
        for block in gate_up
    ]
    order = (own - jnp.arange(peers)) % peers
    partial = jnp.stack(partial)[order]
    summed = exchanged(partial, "tp").astype(jnp.float32).sum(axis=0)
    gate_sum, up_sum = summed[:, :hid], summed[:, hid:]
    hidden = (jax.nn.silu(gate_sum) * up_sum).astype(jnp.bfloat16)
    hidden = from_everyone(hidden, "tp")
    result = jnp.einsum(
        "qrh,qhn->rn",
        hidden,
        w_down[0].reshape(peers, hid, width),
        preferred_element_type=jnp.float32,
    ).astype(jnp.bfloat16)
    tiles = result.reshape(expert_count, capacity * width // LANES, LANES)
    returned = exchanged(tiles, EP).reshape(rows, width)

    picked = [
        jnp.dot(
            (position_of[:, k, None] == slots[None, :]).astype(jnp.bfloat16),
            returned,
            preferred_element_type=jnp.float32,
        )
        for k in range(TOP_K)
    ]
    share_weight = (
        group_weight[:, None] * expert_weight / jnp.sum(expert_weight, axis=1, keepdims=True)
    )
    routed = share_weight[:, 0, None] * picked[0] + share_weight[:, 1, None] * picked[1]
    mixed = residual_scale * tokens.astype(jnp.float32) + routed
    sums = jnp.stack([jnp.sum(mixed, axis=1), jnp.sum(mixed * mixed, axis=1)])
    sums = from_everyone(sums, "tp").sum(axis=0)
    center = sums[0] / D
    spread = sums[1] / D - center * center
    centered = mixed - center[:, None]
    normed = (
        centered * lax.rsqrt(spread + norm_eps)[:, None] * norm_gain[None, :] + norm_bias[None, :]
    )
    return normed.astype(jnp.bfloat16)


def solution(mesh):
    finer = Mesh(mesh.devices.reshape(16, 4, 2, mesh.shape["tp"]), ("ep_0", "ep_1", "ep_2", "tp"))
    placed = (
        P(EP, "tp"),
        P(EP, None),
        P(EP),
        P(EP, None),
        P(EP, None, "tp"),
        P(EP, None, "tp"),
        P(EP, None, "tp"),
        P("tp"),
        P("tp"),
    )
    return jax.shard_map(
        on_device, mesh=finer, in_specs=placed, out_specs=P(EP, "tp"), check_vma=False
    )
```

```python
import functools

import jax
import jax.numpy as jnp
from jax import lax
from jax.experimental import pallas as pl
from jax.experimental.pallas import tpu as pltpu
from jax.sharding import Mesh
from jax.sharding import PartitionSpec as P

D = 4096
GROUPS = 4
TOP_K = 2
EP = ("ep_0", "ep_1", "ep_2")
LANES = 128
F32 = jnp.float32
BF16 = jnp.bfloat16


residual_scale = 2.0**0.5
norm_eps = 1e-05


def exchanged(tiles, axis):
    return lax.all_to_all(tiles, axis, 0, 0, tiled=True)


def in_vmem(count):
    return [pl.BlockSpec(memory_space=pltpu.VMEM) for _ in range(count)]


def permuted(tiles, axis):
    peers = lax.axis_size(axis)
    own = lax.axis_index(axis)
    result = [lax.dynamic_index_in_dim(tiles, own, 0, keepdims=False)]
    for turn in range(1, peers):
        block = lax.dynamic_index_in_dim(tiles, (own + turn) % peers, 0, keepdims=False)
        moves = [(i, (i + turn) % peers) for i in range(peers)]
        result.append(lax.ppermute(block, axis, moves))
    return result


def positions(ids, capacity):
    count = ids.shape[1]
    rows = [jnp.broadcast_to(ids[k : k + 1, :], (count, count)) for k in range(TOP_K)]
    columns = [r.T for r in rows]
    earlier = lax.broadcasted_iota(jnp.int32, (count, count), 0) < lax.broadcasted_iota(
        jnp.int32, (count, count), 1
    )
    found = []
    for k in range(TOP_K):
        same = sum(
            (jnp.where((c == rows[k]) & earlier, 1.0, 0.0) for c in columns),
            jnp.zeros((count, count), F32),
        )
        before = jnp.sum(same, axis=0, keepdims=True)
        for j in range(k):
            before = before + jnp.where(ids[j : j + 1, :] == ids[k : k + 1, :], 1.0, 0.0)
        found.append(ids[k : k + 1, :] * capacity + before.astype(jnp.int32))
    return found


def send_body(ids_ref, tokens_ref, out_ref, *, capacity):
    rows, count = out_ref.shape[0] * LANES // tokens_ref.shape[1], tokens_ref.shape[0]
    where = positions(ids_ref[...], capacity)
    slots = lax.broadcasted_iota(jnp.int32, (rows, count), 0)
    chosen = (slots == where[0]) | (slots == where[1])
    select = jnp.where(chosen, 1.0, 0.0).astype(BF16)
    outgoing = jnp.dot(select, tokens_ref[...], preferred_element_type=F32)
    out_ref[...] = outgoing.reshape(out_ref.shape).astype(BF16)


def pick_body(ids_ref, group_ref, weight_ref, pick_ref, share_ref, *, capacity):
    rows = pick_ref.shape[2]
    count = ids_ref.shape[1]
    where = positions(ids_ref[...], capacity)
    slots = lax.broadcasted_iota(jnp.int32, (rows, count), 0)
    weight = weight_ref[...]
    total = weight[0:1, :] + weight[1:2, :]
    for k in range(TOP_K):
        pick_ref[k] = jnp.where(slots == where[k], 1.0, 0.0).T.astype(BF16)
        share = group_ref[...] * weight[k : k + 1, :] / total
        share_ref[k] = jnp.broadcast_to(share, (count, count)).T


def pack_body(own_ref, *refs):
    out_ref = refs[-1]
    half = out_ref.shape[1]
    hid = out_ref.shape[2] // 2
    for t, block in enumerate(refs[:-1]):
        out_ref[t, :, :hid] = block[:half, :]
        out_ref[t, :, hid:] = block[half:, :]


def partial_body(own_ref, rows_ref, weights_ref, out_ref):
    peers = out_ref.shape[0]
    own = own_ref[0]
    for t in range(peers):
        target = lax.rem(own - t + peers, peers)
        out_ref[target] = jnp.dot(
            rows_ref[...], weights_ref[t], preferred_element_type=F32
        ).astype(BF16)


def hidden_body(sums_ref, out_ref):
    peers, _, hid = out_ref.shape
    total = sums_ref[0].astype(F32)
    for q in range(1, peers):
        total = total + sums_ref[q].astype(F32)
    gate, up = total[:, :hid], total[:, hid:]
    hidden = (gate / (1.0 + jnp.exp(-gate)) * up).astype(BF16)
    for q in range(peers):
        out_ref[q] = hidden


def down_body(hidden_ref, weights_ref, out_ref):
    peers, rows, _ = hidden_ref.shape
    width = weights_ref.shape[1]
    step = rows // 3
    for i in range(3):
        at = pl.ds(i * step, step)
        hidden = jnp.concatenate([hidden_ref[q, at, :] for q in range(peers)], axis=1)
        result = jnp.dot(hidden, weights_ref[...], preferred_element_type=F32)
        tiles = width // LANES
        out_ref[pl.ds(i * step * tiles, step * tiles), :] = result.reshape(
            step * tiles, LANES
        ).astype(BF16)


def mix_body(returned_ref, pick_ref, share_ref, tokens_ref, mixed_ref, sums_ref):
    routed = [
        share_ref[k][:, 0:1]
        * jnp.dot(pick_ref[k], returned_ref[...], preferred_element_type=F32)
        for k in range(TOP_K)
    ]
    mixed = residual_scale * tokens_ref[...].astype(F32) + (routed[0] + routed[1])
    mixed_ref[...] = mixed
    first = jnp.sum(mixed, axis=1, keepdims=True)
    second = jnp.sum(mixed * mixed, axis=1, keepdims=True)
    count = mixed.shape[0]
    lane = lax.broadcasted_iota(jnp.int32, (count, count), 1)
    both = jnp.where(lane == 0, first, jnp.where(lane == 1, second, 0.0)).T[:8, :]
    for q in range(sums_ref.shape[0]):
        sums_ref[q] = both


def norm_body(mixed_ref, sums_ref, gain_ref, bias_ref, out_ref):
    total = sums_ref[0]
    for q in range(1, sums_ref.shape[0]):
        total = total + sums_ref[q]
    center = total[0:1, :] / D
    spread = total[1:2, :] / D - center * center
    scale = lax.rsqrt(spread + norm_eps)
    count = out_ref.shape[0]
    center = jnp.broadcast_to(center, (count, count)).T[:, 0:1]
    scale = jnp.broadcast_to(scale, (count, count)).T[:, 0:1]
    normed = (mixed_ref[...] - center) * scale * gain_ref[...] + bias_ref[...]
    out_ref[...] = normed.astype(BF16)


def on_device(
    tokens, expert_ids, group_weight, expert_weight, w_gate, w_up, w_down, norm_gain, norm_bias
):
    tok_count, width = tokens.shape
    expert_count = lax.axis_size(EP)
    peers = lax.axis_size("tp")
    hid = w_gate.shape[2]
    capacity = min(tok_count // GROUPS, 3 * TOP_K * tok_count // (2 * expert_count))
    rows = expert_count * capacity
    tiles = rows * width // LANES
    ids = expert_ids.T
    own = lax.axis_index("tp").astype(jnp.int32).reshape(1)
    smem = pl.BlockSpec(memory_space=pltpu.SMEM)

    outgoing = pl.pallas_call(
        functools.partial(send_body, capacity=capacity),
        out_shape=jax.ShapeDtypeStruct((tiles, LANES), BF16),
        compiler_params=pltpu.CompilerParams(vmem_limit_bytes=8 << 20),
        name="send",
    )(ids, tokens)
    arrived = exchanged(outgoing.reshape(expert_count, tiles // expert_count, LANES), EP)

    gate_up = jnp.concatenate(
        [w_gate.reshape(peers, width, hid), w_up.reshape(peers, width, hid)], axis=1
    )
    blocks = permuted(gate_up, "tp")
    packed = pl.pallas_call(
        pack_body,
        in_specs=[smem, *in_vmem(peers)],
        out_specs=in_vmem(1)[0],
        out_shape=jax.ShapeDtypeStruct((peers, width, 2 * hid), BF16),
        compiler_params=pltpu.CompilerParams(vmem_limit_bytes=10 << 20),
        name="pack",
    )(own, *blocks)
    pick, share = pl.pallas_call(
        functools.partial(pick_body, capacity=capacity),
        out_specs=in_vmem(2),
        out_shape=(
            jax.ShapeDtypeStruct((TOP_K, tok_count, rows), BF16),
            jax.ShapeDtypeStruct((TOP_K, tok_count, tok_count), F32),
        ),
        compiler_params=pltpu.CompilerParams(vmem_limit_bytes=4 << 20),
        name="pick",
    )(ids, group_weight[None, :], expert_weight.T)

    packed, pick, share = lax.optimization_barrier((packed, pick, share))
    partial = pl.pallas_call(
        partial_body,
        in_specs=[smem, *in_vmem(2)],
        out_specs=in_vmem(1)[0],
        out_shape=jax.ShapeDtypeStruct((peers, rows, 2 * hid), BF16),
        compiler_params=pltpu.CompilerParams(vmem_limit_bytes=10 << 20),
        name="partial",
    )(own, arrived.reshape(rows, width), packed)
    summed = exchanged(partial, "tp")
    hidden = pl.pallas_call(
        hidden_body,
        in_specs=in_vmem(1),
        out_specs=in_vmem(1)[0],
        out_shape=jax.ShapeDtypeStruct((peers, rows, hid), BF16),
        compiler_params=pltpu.CompilerParams(vmem_limit_bytes=6 << 20),
        name="hidden",
    )(summed)
    hidden = exchanged(hidden, "tp")
    result = pl.pallas_call(
        down_body,
        in_specs=in_vmem(2),
        out_specs=in_vmem(1)[0],
        out_shape=jax.ShapeDtypeStruct((tiles, LANES), BF16),
        compiler_params=pltpu.CompilerParams(vmem_limit_bytes=8 << 20),
        name="down",
    )(hidden, w_down[0])
    returned = exchanged(result.reshape(expert_count, tiles // expert_count, LANES), EP)
    mixed, sums = pl.pallas_call(
        mix_body,
        in_specs=in_vmem(4),
        out_specs=in_vmem(2),
        out_shape=(
            jax.ShapeDtypeStruct((tok_count, width), F32),
            jax.ShapeDtypeStruct((peers, 8, tok_count), F32),
        ),
        compiler_params=pltpu.CompilerParams(vmem_limit_bytes=8 << 20),
        name="mix",
    )(returned.reshape(rows, width), pick, share, tokens)
    sums = exchanged(sums, "tp")
    return pl.pallas_call(
        norm_body,
        out_shape=jax.ShapeDtypeStruct((tok_count, width), BF16),
        compiler_params=pltpu.CompilerParams(vmem_limit_bytes=4 << 20),
        name="norm",
    )(mixed, sums, norm_gain[None, :], norm_bias[None, :])


def solution(mesh):
    finer = Mesh(mesh.devices.reshape(16, 4, 2, mesh.shape["tp"]), ("ep_0", "ep_1", "ep_2", "tp"))
    placed = (
        P(EP, "tp"),
        P(EP, None),
        P(EP),
        P(EP, None),
        P(EP, None, "tp"),
        P(EP, None, "tp"),
        P(EP, None, "tp"),
        P("tp"),
        P("tp"),
    )
    return jax.shard_map(
        on_device, mesh=finer, in_specs=placed, out_specs=P(EP, "tp"), check_vma=False
    )
```

```python
import functools

import jax
import jax.numpy as jnp
from jax import lax
from jax.experimental import pallas as pl
from jax.experimental.pallas import tpu as pltpu
from jax.sharding import Mesh
from jax.sharding import PartitionSpec as P

D = 4096
GROUPS = 4
TOP_K = 2
EP = ("ep_0", "ep_1", "ep_2")
LANES = 128
CHUNKS = 3
F32 = jnp.float32
BF16 = jnp.bfloat16


residual_scale = 2.0**0.5
norm_eps = 1e-05


def exchanged(tiles, axis):
    return lax.all_to_all(tiles, axis, 0, 0, tiled=True)


def in_vmem(count):
    return [pl.BlockSpec(memory_space=pltpu.VMEM) for _ in range(count)]


def permuted(tiles, axis):
    peers = lax.axis_size(axis)
    own = lax.axis_index(axis)
    result = [lax.dynamic_index_in_dim(tiles, own, 0, keepdims=False)]
    for turn in range(1, peers):
        block = lax.dynamic_index_in_dim(tiles, (own + turn) % peers, 0, keepdims=False)
        moves = [(i, (i + turn) % peers) for i in range(peers)]
        result.append(lax.ppermute(block, axis, moves))
    return result


def positions(ids, capacity):
    count = ids.shape[1]
    rows = [jnp.broadcast_to(ids[k : k + 1, :], (count, count)) for k in range(TOP_K)]
    columns = [r.T for r in rows]
    earlier = lax.broadcasted_iota(jnp.int32, (count, count), 0) < lax.broadcasted_iota(
        jnp.int32, (count, count), 1
    )
    found = []
    for k in range(TOP_K):
        same = sum(
            (jnp.where((c == rows[k]) & earlier, 1.0, 0.0) for c in columns),
            jnp.zeros((count, count), F32),
        )
        before = jnp.sum(same, axis=0, keepdims=True)
        for j in range(k):
            before = before + jnp.where(ids[j : j + 1, :] == ids[k : k + 1, :], 1.0, 0.0)
        found.append(ids[k : k + 1, :] * capacity + before.astype(jnp.int32))
    return found


def send_body(ids_hbm, tokens_hbm, out_ref, ids_ref, tokens_ref, sems, *, capacity):
    fetch_ids = pltpu.make_async_copy(ids_hbm, ids_ref, sems.at[0])
    fetch_tokens = pltpu.make_async_copy(tokens_hbm, tokens_ref, sems.at[1])
    fetch_ids.start()
    fetch_tokens.start()
    rows, count = out_ref.shape[0] * LANES // tokens_ref.shape[1], tokens_ref.shape[0]
    slots = lax.broadcasted_iota(jnp.int32, (rows, count), 0)
    fetch_ids.wait()
    where = positions(ids_ref[...], capacity)
    chosen = (slots == where[0]) | (slots == where[1])
    select = jnp.where(chosen, 1.0, 0.0).astype(BF16)
    fetch_tokens.wait()
    outgoing = jnp.dot(select, tokens_ref[...], preferred_element_type=F32)
    out_ref[...] = outgoing.reshape(out_ref.shape).astype(BF16)


def pick_body(ids_ref, group_ref, weight_ref, pick_ref, share_ref, *, capacity):
    rows = pick_ref.shape[2]
    count = ids_ref.shape[1]
    where = positions(ids_ref[...], capacity)
    slots = lax.broadcasted_iota(jnp.int32, (rows, count), 0)
    weight = weight_ref[...]
    total = weight[0:1, :] + weight[1:2, :]
    for k in range(TOP_K):
        pick_ref[k] = jnp.where(slots == where[k], 1.0, 0.0).T.astype(BF16)
        share = group_ref[...] * weight[k : k + 1, :] / total
        share_ref[k] = jnp.broadcast_to(share, (count, count)).T


def pack_body(own_ref, *refs):
    out_ref = refs[-1]
    half = out_ref.shape[1]
    hid = out_ref.shape[2] // 2
    for t, block in enumerate(refs[:-1]):
        out_ref[t, :, :hid] = block[:half, :]
        out_ref[t, :, hid:] = block[half:, :]


def partial_body(own_ref, tiles_hbm, weights_ref, out_ref, tiles_ref, sems):
    peers, rows, _ = out_ref.shape
    chunks = tiles_ref.shape[0]
    step, width = rows // chunks, weights_ref.shape[1]
    own = own_ref[0]
    fetches = [
        pltpu.make_async_copy(
            tiles_hbm.at[pl.ds(i * tiles_ref.shape[1], tiles_ref.shape[1])],
            tiles_ref.at[i],
            sems.at[i],
        )
        for i in range(chunks)
    ]
    for f in fetches:
        f.start()
    for i, f in enumerate(fetches):
        f.wait()
        block = tiles_ref[i].astype(F32).reshape(step, width).astype(BF16)
        for t in range(peers):
            target = lax.rem(own - t + peers, peers)
            out_ref[target, pl.ds(i * step, step), :] = jnp.dot(
                block, weights_ref[t], preferred_element_type=F32
            ).astype(BF16)


def hidden_body(sums_ref, out_ref):
    peers, _, hid = out_ref.shape
    total = sums_ref[0].astype(F32)
    for q in range(1, peers):
        total = total + sums_ref[q].astype(F32)
    gate, up = total[:, :hid], total[:, hid:]
    hidden = (gate / (1.0 + jnp.exp(-gate)) * up).astype(BF16)
    for q in range(peers):
        out_ref[q] = hidden


def down_body(hidden_ref, weights_ref, out_ref):
    peers, rows, _ = hidden_ref.shape
    width = weights_ref.shape[1]
    step = rows // 3
    for i in range(3):
        at = pl.ds(i * step, step)
        hidden = jnp.concatenate([hidden_ref[q, at, :] for q in range(peers)], axis=1)
        result = jnp.dot(hidden, weights_ref[...], preferred_element_type=F32)
        tiles = width // LANES
        out_ref[pl.ds(i * step * tiles, step * tiles), :] = result.reshape(
            step * tiles, LANES
        ).astype(BF16)


def mix_body(returned_ref, pick_ref, share_ref, tokens_ref, mixed_ref, sums_ref):
    routed = [
        share_ref[k][:, 0:1]
        * jnp.dot(pick_ref[k], returned_ref[...], preferred_element_type=F32)
        for k in range(TOP_K)
    ]
    mixed = residual_scale * tokens_ref[...].astype(F32) + (routed[0] + routed[1])
    mixed_ref[...] = mixed
    first = jnp.sum(mixed, axis=1, keepdims=True)
    second = jnp.sum(mixed * mixed, axis=1, keepdims=True)
    count = mixed.shape[0]
    lane = lax.broadcasted_iota(jnp.int32, (count, count), 1)
    both = jnp.where(lane == 0, first, jnp.where(lane == 1, second, 0.0)).T[:8, :]
    for q in range(sums_ref.shape[0]):
        sums_ref[q] = both


def norm_body(mixed_ref, sums_ref, gain_ref, bias_ref, out_ref):
    total = sums_ref[0]
    for q in range(1, sums_ref.shape[0]):
        total = total + sums_ref[q]
    center = total[0:1, :] / D
    spread = total[1:2, :] / D - center * center
    scale = lax.rsqrt(spread + norm_eps)
    count = out_ref.shape[0]
    center = jnp.broadcast_to(center, (count, count)).T[:, 0:1]
    scale = jnp.broadcast_to(scale, (count, count)).T[:, 0:1]
    normed = (mixed_ref[...] - center) * scale * gain_ref[...] + bias_ref[...]
    out_ref[...] = normed.astype(BF16)


def on_device(
    tokens, expert_ids, group_weight, expert_weight, w_gate, w_up, w_down, norm_gain, norm_bias
):
    tok_count, width = tokens.shape
    expert_count = lax.axis_size(EP)
    peers = lax.axis_size("tp")
    hid = w_gate.shape[2]
    capacity = min(tok_count // GROUPS, 3 * TOP_K * tok_count // (2 * expert_count))
    rows = expert_count * capacity
    tiles = rows * width // LANES
    ids = expert_ids.T
    own = lax.axis_index("tp").astype(jnp.int32).reshape(1)
    smem = pl.BlockSpec(memory_space=pltpu.SMEM)

    outgoing = pl.pallas_call(
        functools.partial(send_body, capacity=capacity),
        in_specs=[pl.BlockSpec(memory_space=pltpu.HBM)] * 2,
        out_shape=jax.ShapeDtypeStruct((tiles, LANES), BF16),
        scratch_shapes=[
            pltpu.VMEM(ids.shape, ids.dtype),
            pltpu.VMEM(tokens.shape, tokens.dtype),
            pltpu.SemaphoreType.DMA((2,)),
        ],
        compiler_params=pltpu.CompilerParams(vmem_limit_bytes=60 << 20),
        name="send",
    )(ids, tokens)
    arrived = exchanged(outgoing.reshape(expert_count, tiles // expert_count, LANES), EP)

    gate_up = jnp.concatenate(
        [w_gate.reshape(peers, width, hid), w_up.reshape(peers, width, hid)], axis=1
    )
    blocks = permuted(gate_up, "tp")
    packed = pl.pallas_call(
        pack_body,
        in_specs=[smem, *in_vmem(peers)],
        out_specs=in_vmem(1)[0],
        out_shape=jax.ShapeDtypeStruct((peers, width, 2 * hid), BF16),
        compiler_params=pltpu.CompilerParams(vmem_limit_bytes=6 << 20),
        name="pack",
    )(own, *blocks)
    pick, share = pl.pallas_call(
        functools.partial(pick_body, capacity=capacity),
        out_specs=in_vmem(2),
        out_shape=(
            jax.ShapeDtypeStruct((TOP_K, tok_count, rows), BF16),
            jax.ShapeDtypeStruct((TOP_K, tok_count, tok_count), F32),
        ),
        compiler_params=pltpu.CompilerParams(vmem_limit_bytes=2 << 20),
        name="pick",
    )(ids, group_weight[None, :], expert_weight.T)

    packed, pick, share = lax.optimization_barrier((packed, pick, share))
    partial = pl.pallas_call(
        partial_body,
        in_specs=[smem, pl.BlockSpec(memory_space=pl.ANY), *in_vmem(1)],
        out_specs=in_vmem(1)[0],
        out_shape=jax.ShapeDtypeStruct((peers, rows, 2 * hid), BF16),
        scratch_shapes=[
            pltpu.VMEM((CHUNKS, tiles // CHUNKS, LANES), BF16),
            pltpu.SemaphoreType.DMA((CHUNKS,)),
        ],
        compiler_params=pltpu.CompilerParams(vmem_limit_bytes=6 << 20),
        name="partial",
    )(own, arrived.reshape(tiles, LANES), packed)
    summed = exchanged(partial, "tp")
    hidden = pl.pallas_call(
        hidden_body,
        in_specs=in_vmem(1),
        out_specs=in_vmem(1)[0],
        out_shape=jax.ShapeDtypeStruct((peers, rows, hid), BF16),
        compiler_params=pltpu.CompilerParams(vmem_limit_bytes=3 << 20),
        name="hidden",
    )(summed)
    hidden = exchanged(hidden, "tp")
    result = pl.pallas_call(
        down_body,
        in_specs=in_vmem(2),
        out_specs=in_vmem(1)[0],
        out_shape=jax.ShapeDtypeStruct((tiles, LANES), BF16),
        compiler_params=pltpu.CompilerParams(vmem_limit_bytes=4 << 20),
        name="down",
    )(hidden, w_down[0])
    returned = exchanged(result.reshape(expert_count, tiles // expert_count, LANES), EP)
    mixed, sums = pl.pallas_call(
        mix_body,
        in_specs=in_vmem(4),
        out_specs=in_vmem(2),
        out_shape=(
            jax.ShapeDtypeStruct((tok_count, width), F32),
            jax.ShapeDtypeStruct((peers, 8, tok_count), F32),
        ),
        compiler_params=pltpu.CompilerParams(vmem_limit_bytes=4 << 20),
        name="mix",
    )(returned.reshape(rows, width), pick, share, tokens)
    sums = exchanged(sums, "tp")
    return pl.pallas_call(
        norm_body,
        out_shape=jax.ShapeDtypeStruct((tok_count, width), BF16),
        compiler_params=pltpu.CompilerParams(vmem_limit_bytes=2 << 20),
        name="norm",
    )(mixed, sums, norm_gain[None, :], norm_bias[None, :])


def solution(mesh):
    finer = Mesh(mesh.devices.reshape(16, 4, 2, mesh.shape["tp"]), ("ep_0", "ep_1", "ep_2", "tp"))
    placed = (
        P(EP, "tp"),
        P(EP, None),
        P(EP),
        P(EP, None),
        P(EP, None, "tp"),
        P(EP, None, "tp"),
        P(EP, None, "tp"),
        P("tp"),
        P("tp"),
    )
    return jax.shard_map(
        on_device, mesh=finer, in_specs=placed, out_specs=P(EP, "tp"), check_vma=False
    )
```

```python
import functools

import jax
import jax.numpy as jnp
from jax import lax
from jax.experimental import pallas as pl
from jax.experimental.pallas import tpu as pltpu
from jax.sharding import Mesh
from jax.sharding import PartitionSpec as P

D = 4096
GROUPS = 4
TOP_K = 2
EP = ("ep_0", "ep_1", "ep_2")
LANES = 128
CHUNKS = 3
F32 = jnp.float32
BF16 = jnp.bfloat16


residual_scale = 2.0**0.5
norm_eps = 1e-05


def exchanged(tiles, axis):
    return lax.all_to_all(tiles, axis, 0, 0, tiled=True)


def in_vmem(count):
    return [pl.BlockSpec(memory_space=pltpu.VMEM) for _ in range(count)]


def permuted(tiles, axis):
    peers = lax.axis_size(axis)
    own = lax.axis_index(axis)
    result = [lax.dynamic_index_in_dim(tiles, own, 0, keepdims=False)]
    for turn in range(1, peers):
        block = lax.dynamic_index_in_dim(tiles, (own + turn) % peers, 0, keepdims=False)
        moves = [(i, (i + turn) % peers) for i in range(peers)]
        result.append(lax.ppermute(block, axis, moves))
    return result


def positions(ids, capacity):
    count = ids.shape[1]
    rows = [jnp.broadcast_to(ids[k : k + 1, :], (count, count)) for k in range(TOP_K)]
    columns = [r.T for r in rows]
    earlier = lax.broadcasted_iota(jnp.int32, (count, count), 0) < lax.broadcasted_iota(
        jnp.int32, (count, count), 1
    )
    found = []
    for k in range(TOP_K):
        same = sum(
            (jnp.where((c == rows[k]) & earlier, 1.0, 0.0) for c in columns),
            jnp.zeros((count, count), F32),
        )
        before = jnp.sum(same, axis=0, keepdims=True)
        for j in range(k):
            before = before + jnp.where(ids[j : j + 1, :] == ids[k : k + 1, :], 1.0, 0.0)
        found.append(ids[k : k + 1, :] * capacity + before.astype(jnp.int32))
    return found


def send_body(ids_hbm, tokens_hbm, out_hbm, ids_ref, tokens_ref, out_ref, sems, *, capacity):
    fetch_ids = pltpu.make_async_copy(ids_hbm, ids_ref, sems.at[0])
    fetch_tokens = pltpu.make_async_copy(tokens_hbm, tokens_ref, sems.at[1])
    fetch_ids.start()
    fetch_tokens.start()
    chunks, length, _ = out_ref.shape
    count, width = tokens_ref.shape
    step = length * LANES // width
    slots = lax.broadcasted_iota(jnp.int32, (step, count), 0)
    fetch_ids.wait()
    where = positions(ids_ref[...], capacity)
    select = []
    for i in range(chunks):
        chosen = (slots == where[0] - i * step) | (slots == where[1] - i * step)
        select.append(jnp.where(chosen, 1.0, 0.0).astype(BF16))
    fetch_tokens.wait()
    stores = []
    for i in range(chunks):
        outgoing = jnp.dot(select[i], tokens_ref[...], preferred_element_type=F32)
        out_ref[i] = outgoing.reshape(length, LANES).astype(BF16)
        store = pltpu.make_async_copy(
            out_ref.at[i], out_hbm.at[pl.ds(i * length, length)], sems.at[2 + i]
        )
        store.start()
        stores.append(store)
    for store in stores:
        store.wait()


def pick_body(ids_ref, group_ref, weight_ref, pick_ref, share_ref, *, capacity):
    rows = pick_ref.shape[2]
    count = ids_ref.shape[1]
    where = positions(ids_ref[...], capacity)
    slots = lax.broadcasted_iota(jnp.int32, (rows, count), 0)
    weight = weight_ref[...]
    total = weight[0:1, :] + weight[1:2, :]
    for k in range(TOP_K):
        pick_ref[k] = jnp.where(slots == where[k], 1.0, 0.0).T.astype(BF16)
        share = group_ref[...] * weight[k : k + 1, :] / total
        share_ref[k] = jnp.broadcast_to(share, (count, count)).T


def pack_body(own_ref, *refs):
    out_ref = refs[-1]
    half = out_ref.shape[1]
    hid = out_ref.shape[2] // 2
    for t, block in enumerate(refs[:-1]):
        out_ref[t, :, :hid] = block[:half, :]
        out_ref[t, :, hid:] = block[half:, :]


def partial_body(own_ref, tiles_ref, weights_ref, out_ref):
    peers, rows, _ = out_ref.shape
    width = weights_ref.shape[1]
    step = rows // CHUNKS
    length = step * width // LANES
    own = own_ref[0]
    for i in range(CHUNKS):
        block = tiles_ref[pl.ds(i * length, length), :].astype(F32)
        block = block.reshape(step, width).astype(BF16)
        for t in range(peers):
            target = lax.rem(own - t + peers, peers)
            out_ref[target, pl.ds(i * step, step), :] = jnp.dot(
                block, weights_ref[t], preferred_element_type=F32
            ).astype(BF16)


def hidden_body(sums_ref, out_ref):
    peers, _, hid = out_ref.shape
    total = sums_ref[0].astype(F32)
    for q in range(1, peers):
        total = total + sums_ref[q].astype(F32)
    gate, up = total[:, :hid], total[:, hid:]
    hidden = (gate / (1.0 + jnp.exp(-gate)) * up).astype(BF16)
    for q in range(peers):
        out_ref[q] = hidden


def down_body(hidden_ref, weights_ref, out_ref):
    peers, rows, _ = hidden_ref.shape
    width = weights_ref.shape[1]
    step = rows // 3
    for i in range(3):
        at = pl.ds(i * step, step)
        hidden = jnp.concatenate([hidden_ref[q, at, :] for q in range(peers)], axis=1)
        result = jnp.dot(hidden, weights_ref[...], preferred_element_type=F32)
        tiles = width // LANES
        out_ref[pl.ds(i * step * tiles, step * tiles), :] = result.reshape(
            step * tiles, LANES
        ).astype(BF16)


def mix_body(tiles_ref, pick_ref, share_ref, tokens_ref, mixed_ref, sums_ref):
    count, width = tokens_ref.shape
    rows = tiles_ref.shape[0] * LANES // width
    step = rows // CHUNKS
    length = step * width // LANES
    routed = [jnp.zeros((count, width), F32) for _ in range(TOP_K)]
    for i in range(CHUNKS):
        block = tiles_ref[pl.ds(i * length, length), :].astype(F32)
        block = block.reshape(step, width).astype(BF16)
        for k in range(TOP_K):
            routed[k] = routed[k] + jnp.dot(
                pick_ref[k, :, i * step : (i + 1) * step], block, preferred_element_type=F32
            )
    routed = [share_ref[k][:, 0:1] * routed[k] for k in range(TOP_K)]
    mixed = residual_scale * tokens_ref[...].astype(F32) + (routed[0] + routed[1])
    mixed_ref[...] = mixed
    first = jnp.sum(mixed, axis=1, keepdims=True)
    second = jnp.sum(mixed * mixed, axis=1, keepdims=True)
    lane = lax.broadcasted_iota(jnp.int32, (count, count), 1)
    both = jnp.where(lane == 0, first, jnp.where(lane == 1, second, 0.0)).T[:8, :]
    for q in range(sums_ref.shape[0]):
        sums_ref[q] = both


def norm_body(mixed_ref, sums_ref, gain_ref, bias_ref, out_ref):
    total = sums_ref[0]
    for q in range(1, sums_ref.shape[0]):
        total = total + sums_ref[q]
    center = total[0:1, :] / D
    spread = total[1:2, :] / D - center * center
    scale = lax.rsqrt(spread + norm_eps)
    count = out_ref.shape[0]
    center = jnp.broadcast_to(center, (count, count)).T[:, 0:1]
    scale = jnp.broadcast_to(scale, (count, count)).T[:, 0:1]
    normed = (mixed_ref[...] - center) * scale * gain_ref[...] + bias_ref[...]
    out_ref[...] = normed.astype(BF16)


def on_device(
    tokens, expert_ids, group_weight, expert_weight, w_gate, w_up, w_down, norm_gain, norm_bias
):
    tok_count, width = tokens.shape
    expert_count = lax.axis_size(EP)
    peers = lax.axis_size("tp")
    hid = w_gate.shape[2]
    capacity = min(tok_count // GROUPS, 3 * TOP_K * tok_count // (2 * expert_count))
    rows = expert_count * capacity
    tiles = rows * width // LANES
    ids = expert_ids.T
    own = lax.axis_index("tp").astype(jnp.int32).reshape(1)
    smem = pl.BlockSpec(memory_space=pltpu.SMEM)

    outgoing = pl.pallas_call(
        functools.partial(send_body, capacity=capacity),
        in_specs=[pl.BlockSpec(memory_space=pltpu.HBM)] * 2,
        out_specs=pl.BlockSpec(memory_space=pltpu.HBM),
        out_shape=jax.ShapeDtypeStruct((tiles, LANES), BF16),
        scratch_shapes=[
            pltpu.VMEM(ids.shape, ids.dtype),
            pltpu.VMEM(tokens.shape, tokens.dtype),
            pltpu.VMEM((CHUNKS, tiles // CHUNKS, LANES), BF16),
            pltpu.SemaphoreType.DMA((2 + CHUNKS,)),
        ],
        compiler_params=pltpu.CompilerParams(vmem_limit_bytes=67_000_000),
        name="send",
    )(ids, tokens)
    arrived = exchanged(outgoing.reshape(expert_count, tiles // expert_count, LANES), EP)

    gate_up = jnp.concatenate(
        [w_gate.reshape(peers, width, hid), w_up.reshape(peers, width, hid)], axis=1
    )
    blocks = permuted(gate_up, "tp")
    packed = pl.pallas_call(
        pack_body,
        in_specs=[smem, *in_vmem(peers)],
        out_specs=in_vmem(1)[0],
        out_shape=jax.ShapeDtypeStruct((peers, width, 2 * hid), BF16),
        compiler_params=pltpu.CompilerParams(vmem_limit_bytes=6 << 20),
        name="pack",
    )(own, *blocks)
    pick, share = pl.pallas_call(
        functools.partial(pick_body, capacity=capacity),
        out_specs=in_vmem(2),
        out_shape=(
            jax.ShapeDtypeStruct((TOP_K, tok_count, rows), BF16),
            jax.ShapeDtypeStruct((TOP_K, tok_count, tok_count), F32),
        ),
        compiler_params=pltpu.CompilerParams(vmem_limit_bytes=2 << 20),
        name="pick",
    )(ids, group_weight[None, :], expert_weight.T)

    packed, pick, share = lax.optimization_barrier((packed, pick, share))
    partial = pl.pallas_call(
        partial_body,
        in_specs=[smem, *in_vmem(2)],
        out_specs=in_vmem(1)[0],
        out_shape=jax.ShapeDtypeStruct((peers, rows, 2 * hid), BF16),
        compiler_params=pltpu.CompilerParams(vmem_limit_bytes=5 << 20),
        name="partial",
    )(own, arrived.reshape(tiles, LANES), packed)
    summed = exchanged(partial, "tp")
    hidden = pl.pallas_call(
        hidden_body,
        in_specs=in_vmem(1),
        out_specs=in_vmem(1)[0],
        out_shape=jax.ShapeDtypeStruct((peers, rows, hid), BF16),
        compiler_params=pltpu.CompilerParams(vmem_limit_bytes=3 << 20),
        name="hidden",
    )(summed)
    hidden = exchanged(hidden, "tp")
    result = pl.pallas_call(
        down_body,
        in_specs=in_vmem(2),
        out_specs=in_vmem(1)[0],
        out_shape=jax.ShapeDtypeStruct((tiles, LANES), BF16),
        compiler_params=pltpu.CompilerParams(vmem_limit_bytes=4 << 20),
        name="down",
    )(hidden, w_down[0])
    returned = exchanged(result.reshape(expert_count, tiles // expert_count, LANES), EP)
    mixed, sums = pl.pallas_call(
        mix_body,
        in_specs=in_vmem(4),
        out_specs=in_vmem(2),
        out_shape=(
            jax.ShapeDtypeStruct((tok_count, width), F32),
            jax.ShapeDtypeStruct((peers, 8, tok_count), F32),
        ),
        compiler_params=pltpu.CompilerParams(vmem_limit_bytes=4 << 20),
        name="mix",
    )(returned.reshape(tiles, LANES), pick, share, tokens)
    sums = exchanged(sums, "tp")
    return pl.pallas_call(
        norm_body,
        out_shape=jax.ShapeDtypeStruct((tok_count, width), BF16),
        compiler_params=pltpu.CompilerParams(vmem_limit_bytes=2 << 20),
        name="norm",
    )(mixed, sums, norm_gain[None, :], norm_bias[None, :])


def solution(mesh):
    finer = Mesh(mesh.devices.reshape(16, 4, 2, mesh.shape["tp"]), ("ep_0", "ep_1", "ep_2", "tp"))
    placed = (
        P(EP, "tp"),
        P(EP, None),
        P(EP),
        P(EP, None),
        P(EP, None, "tp"),
        P(EP, None, "tp"),
        P(EP, None, "tp"),
        P("tp"),
        P("tp"),
    )
    return jax.shard_map(
        on_device, mesh=finer, in_specs=placed, out_specs=P(EP, "tp"), check_vma=False
    )
```

```python
import functools

import jax
import jax.numpy as jnp
from jax import lax
from jax.experimental import pallas as pl
from jax.experimental.pallas import tpu as pltpu
from jax.sharding import Mesh
from jax.sharding import PartitionSpec as P

D = 4096
GROUPS = 4
TOP_K = 2
EP = ("ep_0", "ep_1", "ep_2")
CHIPS = ("ep_0", "ep_1")
CORES = 2
LAG = 0
LATE = 1
HELD = (1, 2, 3)
LANES = 128
CHUNKS = 3
F32 = jnp.float32
BF16 = jnp.bfloat16


residual_scale = 2.0**0.5
norm_eps = 1e-05


def exchanged(tiles, axis):
    return lax.all_to_all(tiles, axis, 0, 0, tiled=True)


def in_vmem(count):
    return [pl.BlockSpec(memory_space=pltpu.VMEM) for _ in range(count)]


def permuted(tiles, axis):
    peers = lax.axis_size(axis)
    own = lax.axis_index(axis)
    result = [lax.dynamic_index_in_dim(tiles, own, 0, keepdims=False)]
    for turn in range(1, peers):
        block = lax.dynamic_index_in_dim(tiles, (own + turn) % peers, 0, keepdims=False)
        moves = [(i, (i + turn) % peers) for i in range(peers)]
        result.append(lax.ppermute(block, axis, moves))
    return result


def positions(ids, capacity, core, block):
    count = ids.shape[1]
    rows = [jnp.broadcast_to(ids[k : k + 1, :], (count, count)) for k in range(TOP_K)]
    columns = [r.T for r in rows]
    earlier = lax.broadcasted_iota(jnp.int32, (count, count), 0) < lax.broadcasted_iota(
        jnp.int32, (count, count), 1
    )
    found = []
    for k in range(TOP_K):
        same = sum(
            (jnp.where((c == rows[k]) & earlier, 1.0, 0.0) for c in columns),
            jnp.zeros((count, count), F32),
        )
        before = jnp.sum(same, axis=0, keepdims=True)
        for j in range(k):
            before = before + jnp.where(ids[j : j + 1, :] == ids[k : k + 1, :], 1.0, 0.0)
        chosen = ids[k : k + 1, :]
        chip = lax.shift_right_logical(chosen, 1)
        row = (chip * CORES + block) * capacity + before.astype(jnp.int32)
        found.append(jnp.where((chosen & 1) == core, row, -1))
    return found


def bundle_body(ids_hbm, tokens_hbm, out_ref, ids_ref, sems):
    count = tokens_hbm.shape[0]
    fetch_ids = pltpu.make_async_copy(ids_hbm, ids_ref, sems.at[0])
    fetch_tokens = pltpu.make_async_copy(tokens_hbm, out_ref.at[pl.ds(0, count)], sems.at[1])
    fetch_ids.start()
    fetch_tokens.start()
    extra = out_ref.shape[0] - count
    fetch_ids.wait()
    line = lax.broadcasted_iota(jnp.int32, (extra, count), 0)
    marks = jnp.where(line == 0, ids_ref[0:1, :], ids_ref[1:2, :])
    out_ref[count:, :count] = marks.astype(F32).astype(BF16)
    fetch_tokens.wait()


def hold_body(rows_hbm, *refs):
    del rows_hbm, refs


def send_body(
    core_ref,
    ids_hbm,
    own_hbm,
    peer_hbm,
    out_hbm,
    peer_ids_out,
    ids_ref,
    peer_ids_ref,
    marks_ref,
    tokens_ref,
    out_ref,
    sems,
    *,
    capacity,
    lag,
):
    chunks, length, _ = out_ref.shape
    extra, count = marks_ref.shape
    width = own_hbm.shape[1]
    fetch_ids = [
        pltpu.make_async_copy(ids_hbm, ids_ref, sems.at[0]),
        pltpu.make_async_copy(
            peer_hbm.at[pl.ds(count, extra), pl.ds(0, count)], marks_ref, sems.at[1]
        ),
    ]
    fetch_tokens = [
        pltpu.make_async_copy(
            t.at[pl.ds(0, count)], tokens_ref.at[pl.ds(b * count, count)], sems.at[CORES + b]
        )
        for b, t in enumerate((own_hbm, peer_hbm))
    ]
    for f in fetch_ids + fetch_tokens:
        f.start()
    core = core_ref[0]
    step = length * LANES // width
    slots = lax.broadcasted_iota(jnp.int32, (step, count), 0)
    for f in fetch_ids:
        f.wait()
    peer_ids_ref[...] = marks_ref[...].astype(F32).astype(jnp.int32)[0:TOP_K, :]
    save_ids = pltpu.make_async_copy(peer_ids_ref, peer_ids_out, sems.at[2 * CORES + chunks])
    save_ids.start()
    where = [
        positions(ids[...], capacity, core, b) for b, ids in enumerate((ids_ref, peer_ids_ref))
    ]
    select = []
    for i in range(chunks):
        marks = [
            jnp.where((slots == w[0] - i * step) | (slots == w[1] - i * step), 1.0, 0.0)
            for w in where
        ]
        select.append(jnp.concatenate(marks, axis=1).astype(BF16))
    for f in fetch_tokens:
        f.wait()
    stores = []
    for i in range(chunks):
        outgoing = jnp.dot(select[i], tokens_ref[...], preferred_element_type=F32)
        out_ref[i] = outgoing.reshape(length, LANES).astype(BF16)
        store = pltpu.make_async_copy(
            out_ref.at[i], out_hbm.at[pl.ds(i * length, length)], sems.at[2 * CORES + i]
        )
        store.start()
        stores.append(store)
    for store in stores + [save_ids]:
        store.wait()

    if lag:

        @pl.when(core == LATE)
        def _():
            pl.delay(lag)


def pick_body(core_ref, ids_ref, peer_ids_ref, group_ref, weight_ref, pick_ref, share_ref, *, capacity):
    rows = pick_ref.shape[3]
    count = ids_ref.shape[1]
    core = core_ref[0]
    slots = lax.broadcasted_iota(jnp.int32, (rows, count), 0)
    for b, ids in enumerate((ids_ref, peer_ids_ref)):
        where = positions(ids[...], capacity, core, b)
        for k in range(TOP_K):
            pick_ref[b, k] = jnp.where(slots == where[k], 1.0, 0.0).T.astype(BF16)
    weight = weight_ref[...]
    total = weight[0:1, :] + weight[1:2, :]
    for k in range(TOP_K):
        share = group_ref[...] * weight[k : k + 1, :] / total
        share_ref[k] = jnp.broadcast_to(share, (count, count)).T


def pack_body(own_ref, *refs):
    out_ref = refs[-1]
    half = out_ref.shape[1]
    hid = out_ref.shape[2] // 2
    for t, block in enumerate(refs[:-1]):
        out_ref[t, :, :hid] = block[:half, :]
        out_ref[t, :, hid:] = block[half:, :]


def partial_body(own_ref, tiles_hbm, weights_ref, out_ref, tiles_ref, sems):
    peers, rows, _ = out_ref.shape
    chunks = tiles_ref.shape[0]
    step, width = rows // chunks, weights_ref.shape[1]
    own = own_ref[0]
    fetches = [
        pltpu.make_async_copy(
            tiles_hbm.at[pl.ds(i * tiles_ref.shape[1], tiles_ref.shape[1])],
            tiles_ref.at[i],
            sems.at[i],
        )
        for i in range(chunks)
    ]
    for f in fetches:
        f.start()
    for i, f in enumerate(fetches):
        f.wait()
        block = tiles_ref[i].astype(F32).reshape(step, width).astype(BF16)
        for t in range(peers):
            target = lax.rem(own - t + peers, peers)
            out_ref[target, pl.ds(i * step, step), :] = jnp.dot(
                block, weights_ref[t], preferred_element_type=F32
            ).astype(BF16)


def hidden_body(sums_ref, out_ref):
    peers, _, hid = out_ref.shape
    total = sums_ref[0].astype(F32)
    for q in range(1, peers):
        total = total + sums_ref[q].astype(F32)
    gate, up = total[:, :hid], total[:, hid:]
    hidden = (gate / (1.0 + jnp.exp(-gate)) * up).astype(BF16)
    for q in range(peers):
        out_ref[q] = hidden


def down_body(hidden_ref, weights_ref, out_ref):
    peers, rows, _ = hidden_ref.shape
    width = weights_ref.shape[1]
    step = rows // 3
    for i in range(3):
        at = pl.ds(i * step, step)
        hidden = jnp.concatenate([hidden_ref[q, at, :] for q in range(peers)], axis=1)
        result = jnp.dot(hidden, weights_ref[...], preferred_element_type=F32)
        tiles = width // LANES
        out_ref[pl.ds(i * step * tiles, step * tiles), :] = result.reshape(
            step * tiles, LANES
        ).astype(BF16)


def lend_body(tiles_ref, pick_ref, lent_ref, rows_ref):
    rows, width = rows_ref.shape
    step = rows // CHUNKS
    length = step * width // LANES
    for i in range(CHUNKS):
        block = tiles_ref[pl.ds(i * length, length), :].astype(F32)
        rows_ref[pl.ds(i * step, step), :] = block.reshape(step, width).astype(BF16)
    for k in range(TOP_K):
        lent_ref[k] = jnp.dot(
            pick_ref[1, k], rows_ref[...], preferred_element_type=F32
        ).astype(BF16)


def keep_body(rows_ref, pick_ref, share_ref, tokens_ref, mixed_ref):
    mixed = residual_scale * tokens_ref[...].astype(F32)
    for k in range(TOP_K):
        kept = jnp.dot(pick_ref[0, k], rows_ref[...], preferred_element_type=F32)
        mixed = mixed + share_ref[k][:, 0:1] * kept
    mixed_ref[...] = mixed


def mix_body(part_ref, other_ref, share_ref, mixed_ref, sums_ref):
    mixed = part_ref[...]
    for k in range(TOP_K):
        mixed = mixed + share_ref[k][:, 0:1] * other_ref[k].astype(F32)
    count = mixed.shape[0]
    mixed_ref[...] = mixed
    first = jnp.sum(mixed, axis=1, keepdims=True)
    second = jnp.sum(mixed * mixed, axis=1, keepdims=True)
    lane = lax.broadcasted_iota(jnp.int32, (count, count), 1)
    both = jnp.where(lane == 0, first, jnp.where(lane == 1, second, 0.0)).T[:8, :]
    for q in range(sums_ref.shape[0]):
        sums_ref[q] = both


def norm_body(mixed_ref, sums_ref, gain_ref, bias_ref, out_ref):
    total = sums_ref[0]
    for q in range(1, sums_ref.shape[0]):
        total = total + sums_ref[q]
    center = total[0:1, :] / D
    spread = total[1:2, :] / D - center * center
    scale = lax.rsqrt(spread + norm_eps)
    count = out_ref.shape[0]
    center = jnp.broadcast_to(center, (count, count)).T[:, 0:1]
    scale = jnp.broadcast_to(scale, (count, count)).T[:, 0:1]
    normed = (mixed_ref[...] - center) * scale * gain_ref[...] + bias_ref[...]
    out_ref[...] = normed.astype(BF16)


def on_device(
    tokens, expert_ids, group_weight, expert_weight, w_gate, w_up, w_down, norm_gain, norm_bias
):
    tok_count, width = tokens.shape
    expert_count = lax.axis_size(EP)
    peers = lax.axis_size("tp")
    hid = w_gate.shape[2]
    capacity = min(tok_count // GROUPS, 3 * TOP_K * tok_count // (2 * expert_count))
    rows = expert_count * capacity
    tiles = rows * width // LANES
    chips = expert_count // CORES
    ids = expert_ids.T
    own = lax.axis_index("tp").astype(jnp.int32).reshape(1)
    core = lax.axis_index("ep_2").astype(jnp.int32).reshape(1)
    smem = pl.BlockSpec(memory_space=pltpu.SMEM)
    swap = [(c, CORES - 1 - c) for c in range(CORES)]
    hbm = pl.BlockSpec(memory_space=pl.ANY)
    bundle = pl.pallas_call(
        bundle_body,
        in_specs=[hbm] * 2,
        out_specs=in_vmem(1)[0],
        out_shape=jax.ShapeDtypeStruct((tok_count + 8, width), BF16),
        scratch_shapes=[pltpu.VMEM(ids.shape, ids.dtype), pltpu.SemaphoreType.DMA((2,))],
        compiler_params=pltpu.CompilerParams(vmem_limit_bytes=2 << 20),
        name="bundle",
    )(ids, tokens)
    peer = lax.ppermute(bundle, "ep_2", swap)

    outgoing, peer_ids = pl.pallas_call(
        functools.partial(send_body, capacity=capacity, lag=LAG),
        in_specs=[smem, hbm, hbm, hbm],
        out_specs=[hbm, hbm],
        out_shape=(
            jax.ShapeDtypeStruct((tiles, LANES), BF16),
            jax.ShapeDtypeStruct(ids.shape, ids.dtype),
        ),
        scratch_shapes=[
            pltpu.VMEM(ids.shape, ids.dtype),
            pltpu.VMEM(ids.shape, ids.dtype),
            pltpu.VMEM((8, tok_count), BF16),
            pltpu.VMEM((CORES * tok_count, width), tokens.dtype),
            pltpu.VMEM((CHUNKS, tiles // CHUNKS, LANES), BF16),
            pltpu.SemaphoreType.DMA((2 * CORES + CHUNKS + 1,)),
        ],
        compiler_params=pltpu.CompilerParams(vmem_limit_bytes=6 << 20),
        name="send",
    )(core, ids, bundle, peer)
    def weights_of(w_gate, w_up):
        both = [w.reshape(peers, width, hid) for w in (w_gate, w_up)]
        return permuted(jnp.concatenate(both, axis=1), "tp")

    def packed_of(blocks):
        return pl.pallas_call(
            pack_body,
            in_specs=[smem, *in_vmem(peers)],
            out_specs=in_vmem(1)[0],
            out_shape=jax.ShapeDtypeStruct((peers, width, 2 * hid), BF16),
            compiler_params=pltpu.CompilerParams(vmem_limit_bytes=6 << 20),
            name="pack",
        )(own, *blocks)

    def picked(peer_ids):
        return pl.pallas_call(
            functools.partial(pick_body, capacity=capacity),
            in_specs=[smem, *in_vmem(4)],
            out_specs=in_vmem(2),
            out_shape=(
                jax.ShapeDtypeStruct((CORES, TOP_K, tok_count, rows), BF16),
                jax.ShapeDtypeStruct((TOP_K, tok_count, tok_count), F32),
            ),
            compiler_params=pltpu.CompilerParams(vmem_limit_bytes=3 << 20),
            name="pick",
        )(core, ids, peer_ids, group_weight[None, :], expert_weight.T)

    def partial_of(arrived, blocks, peer_ids):
        packed, pick, share = lax.optimization_barrier((packed_of(blocks), *picked(peer_ids)))
        partial = pl.pallas_call(
            partial_body,
            in_specs=[smem, pl.BlockSpec(memory_space=pl.ANY), *in_vmem(1)],
            out_specs=in_vmem(1)[0],
            out_shape=jax.ShapeDtypeStruct((peers, rows, 2 * hid), BF16),
            scratch_shapes=[
                pltpu.VMEM((CHUNKS, tiles // CHUNKS, LANES), BF16),
                pltpu.SemaphoreType.DMA((CHUNKS,)),
            ],
            compiler_params=pltpu.CompilerParams(vmem_limit_bytes=6 << 20),
            name="partial",
        )(own, arrived.reshape(tiles, LANES), packed)
        return partial, pick, share

    def rows_first(outgoing, peer_ids, w_gate, w_up):
        arrived = exchanged(outgoing, CHIPS)
        return partial_of(arrived, weights_of(w_gate, w_up), peer_ids)

    def weights_first(outgoing, peer_ids, w_gate, w_up):
        blocks = weights_of(w_gate, w_up)
        held = [blocks[t] for t in HELD]
        outgoing = pl.pallas_call(
            hold_body,
            in_specs=[pl.BlockSpec(memory_space=pl.ANY)] * (1 + len(held)),
            out_specs=pl.BlockSpec(memory_space=pl.ANY),
            out_shape=jax.ShapeDtypeStruct(outgoing.shape, outgoing.dtype),
            input_output_aliases={0: 0},
            compiler_params=pltpu.CompilerParams(vmem_limit_bytes=1 << 20),
            name="hold",
        )(outgoing, *held)
        return partial_of(exchanged(outgoing, CHIPS), blocks, peer_ids)

    partial, pick, share = lax.cond(
        core[0] == LATE,
        weights_first,
        rows_first,
        outgoing.reshape(chips, tiles // chips, LANES),
        peer_ids,
        w_gate,
        w_up,
    )
    summed = exchanged(partial, "tp")
    hidden = pl.pallas_call(
        hidden_body,
        in_specs=in_vmem(1),
        out_specs=in_vmem(1)[0],
        out_shape=jax.ShapeDtypeStruct((peers, rows, hid), BF16),
        compiler_params=pltpu.CompilerParams(vmem_limit_bytes=3 << 20),
        name="hidden",
    )(summed)
    hidden = exchanged(hidden, "tp")
    result = pl.pallas_call(
        down_body,
        in_specs=in_vmem(2),
        out_specs=in_vmem(1)[0],
        out_shape=jax.ShapeDtypeStruct((tiles, LANES), BF16),
        compiler_params=pltpu.CompilerParams(vmem_limit_bytes=4 << 20),
        name="down",
    )(hidden, w_down[0])
    returned = exchanged(result.reshape(chips, tiles // chips, LANES), CHIPS)
    lent, kept_rows = pl.pallas_call(
        lend_body,
        in_specs=in_vmem(2),
        out_specs=in_vmem(2),
        out_shape=(
            jax.ShapeDtypeStruct((TOP_K, tok_count, width), BF16),
            jax.ShapeDtypeStruct((rows, width), BF16),
        ),
        compiler_params=pltpu.CompilerParams(vmem_limit_bytes=4 << 20),
        name="lend",
    )(returned.reshape(tiles, LANES), pick)
    other = lax.ppermute(lent, "ep_2", swap)
    part = pl.pallas_call(
        keep_body,
        in_specs=in_vmem(4),
        out_specs=in_vmem(1)[0],
        out_shape=jax.ShapeDtypeStruct((tok_count, width), F32),
        compiler_params=pltpu.CompilerParams(vmem_limit_bytes=4 << 20),
        name="keep",
    )(kept_rows, pick, share, tokens)
    mixed, sums = pl.pallas_call(
        mix_body,
        in_specs=in_vmem(3),
        out_specs=in_vmem(2),
        out_shape=(
            jax.ShapeDtypeStruct((tok_count, width), F32),
            jax.ShapeDtypeStruct((peers, 8, tok_count), F32),
        ),
        compiler_params=pltpu.CompilerParams(vmem_limit_bytes=4 << 20),
        name="mix",
    )(part, other, share)
    sums = exchanged(sums, "tp")
    return pl.pallas_call(
        norm_body,
        out_shape=jax.ShapeDtypeStruct((tok_count, width), BF16),
        compiler_params=pltpu.CompilerParams(vmem_limit_bytes=2 << 20),
        name="norm",
    )(mixed, sums, norm_gain[None, :], norm_bias[None, :])


def solution(mesh):
    finer = Mesh(mesh.devices.reshape(16, 4, 2, mesh.shape["tp"]), ("ep_0", "ep_1", "ep_2", "tp"))
    placed = (
        P(EP, "tp"),
        P(EP, None),
        P(EP),
        P(EP, None),
        P(EP, None, "tp"),
        P(EP, None, "tp"),
        P(EP, None, "tp"),
        P("tp"),
        P("tp"),
    )
    return jax.shard_map(
        on_device, mesh=finer, in_specs=placed, out_specs=P(EP, "tp"), check_vma=False
    )
```

```python
import functools

import jax
import jax.numpy as jnp
from jax import lax
from jax.experimental import pallas as pl
from jax.experimental.pallas import tpu as pltpu
from jax.sharding import Mesh
from jax.sharding import PartitionSpec as P

D = 4096
GROUPS = 4
TOP_K = 2
EP = ("ep_0", "ep_1", "ep_2")
CHIPS = ("ep_0", "ep_1")
CORES = 2
LAG = 0
LATE = 1
HELD = (1, 2, 3)
LANES = 128
CHUNKS = 3
F32 = jnp.float32
BF16 = jnp.bfloat16


residual_scale = 2.0**0.5
norm_eps = 1e-05


def exchanged(tiles, axis):
    return lax.all_to_all(tiles, axis, 0, 0, tiled=True)


def in_vmem(count):
    return [pl.BlockSpec(memory_space=pltpu.VMEM) for _ in range(count)]


def permuted(tiles, axis):
    peers = lax.axis_size(axis)
    own = lax.axis_index(axis)
    result = [lax.dynamic_index_in_dim(tiles, own, 0, keepdims=False)]
    for turn in range(1, peers):
        block = lax.dynamic_index_in_dim(tiles, (own + turn) % peers, 0, keepdims=False)
        moves = [(i, (i + turn) % peers) for i in range(peers)]
        result.append(lax.ppermute(block, axis, moves))
    return result


def positions(ids, capacity, core, block):
    count = ids.shape[1]
    rows = [jnp.broadcast_to(ids[k : k + 1, :], (count, count)) for k in range(TOP_K)]
    columns = [r.T for r in rows]
    earlier = lax.broadcasted_iota(jnp.int32, (count, count), 0) < lax.broadcasted_iota(
        jnp.int32, (count, count), 1
    )
    found = []
    for k in range(TOP_K):
        same = sum(
            (jnp.where((c == rows[k]) & earlier, 1.0, 0.0) for c in columns),
            jnp.zeros((count, count), F32),
        )
        before = jnp.sum(same, axis=0, keepdims=True)
        for j in range(k):
            before = before + jnp.where(ids[j : j + 1, :] == ids[k : k + 1, :], 1.0, 0.0)
        chosen = ids[k : k + 1, :]
        chip = lax.shift_right_logical(chosen, 1)
        row = (chip * CORES + block) * capacity + before.astype(jnp.int32)
        found.append(jnp.where((chosen & 1) == core, row, -1))
    return found


def bundle_body(ids_hbm, tokens_hbm, out_ref, ids_ref, sems):
    count = tokens_hbm.shape[0]
    fetch_ids = pltpu.make_async_copy(ids_hbm, ids_ref, sems.at[0])
    fetch_tokens = pltpu.make_async_copy(tokens_hbm, out_ref.at[pl.ds(0, count)], sems.at[1])
    fetch_ids.start()
    fetch_tokens.start()
    extra = out_ref.shape[0] - count
    fetch_ids.wait()
    line = lax.broadcasted_iota(jnp.int32, (extra, count), 0)
    marks = jnp.where(line == 0, ids_ref[0:1, :], ids_ref[1:2, :])
    out_ref[count:, :count] = marks.astype(F32).astype(BF16)
    fetch_tokens.wait()


def hold_body(rows_hbm, *refs):
    del rows_hbm, refs


def send_body(
    core_ref,
    ids_hbm,
    own_hbm,
    peer_hbm,
    out_hbm,
    peer_ids_out,
    ids_ref,
    peer_ids_ref,
    marks_ref,
    tokens_ref,
    out_ref,
    sems,
    *,
    capacity,
    lag,
):
    chunks, length, _ = out_ref.shape
    extra, count = marks_ref.shape
    width = own_hbm.shape[1]
    fetch_ids = [
        pltpu.make_async_copy(ids_hbm, ids_ref, sems.at[0]),
        pltpu.make_async_copy(
            peer_hbm.at[pl.ds(count, extra), pl.ds(0, count)], marks_ref, sems.at[1]
        ),
    ]
    fetch_tokens = [
        pltpu.make_async_copy(
            t.at[pl.ds(0, count)], tokens_ref.at[pl.ds(b * count, count)], sems.at[CORES + b]
        )
        for b, t in enumerate((own_hbm, peer_hbm))
    ]
    for f in fetch_ids + fetch_tokens:
        f.start()
    core = core_ref[0]
    step = length * LANES // width
    slots = lax.broadcasted_iota(jnp.int32, (step, count), 0)
    for f in fetch_ids:
        f.wait()
    peer_ids_ref[...] = marks_ref[...].astype(F32).astype(jnp.int32)[0:TOP_K, :]
    save_ids = pltpu.make_async_copy(peer_ids_ref, peer_ids_out, sems.at[2 * CORES + chunks])
    save_ids.start()
    where = [
        positions(ids[...], capacity, core, b) for b, ids in enumerate((ids_ref, peer_ids_ref))
    ]
    select = []
    for i in range(chunks):
        marks = [
            jnp.where((slots == w[0] - i * step) | (slots == w[1] - i * step), 1.0, 0.0)
            for w in where
        ]
        select.append(jnp.concatenate(marks, axis=1).astype(BF16))
    for f in fetch_tokens:
        f.wait()
    stores = []
    for i in range(chunks):
        outgoing = jnp.dot(select[i], tokens_ref[...], preferred_element_type=F32)
        out_ref[i] = outgoing.reshape(length, LANES).astype(BF16)
        store = pltpu.make_async_copy(
            out_ref.at[i], out_hbm.at[pl.ds(i * length, length)], sems.at[2 * CORES + i]
        )
        store.start()
        stores.append(store)
    for store in stores + [save_ids]:
        store.wait()

    if lag:

        @pl.when(core == LATE)
        def _():
            pl.delay(lag)


def pick_body(core_ref, ids_ref, peer_ids_ref, group_ref, weight_ref, pick_ref, share_ref, *, capacity):
    rows = pick_ref.shape[3]
    count = ids_ref.shape[1]
    core = core_ref[0]
    slots = lax.broadcasted_iota(jnp.int32, (rows, count), 0)
    for b, ids in enumerate((ids_ref, peer_ids_ref)):
        where = positions(ids[...], capacity, core, b)
        for k in range(TOP_K):
            pick_ref[b, k] = jnp.where(slots == where[k], 1.0, 0.0).T.astype(BF16)
    weight = weight_ref[...]
    total = weight[0:1, :] + weight[1:2, :]
    for k in range(TOP_K):
        share = group_ref[...] * weight[k : k + 1, :] / total
        share_ref[k] = jnp.broadcast_to(share, (count, count)).T


def pack_body(own_ref, *refs):
    out_ref = refs[-1]
    half = out_ref.shape[1]
    hid = out_ref.shape[2] // 2
    for t, block in enumerate(refs[:-1]):
        out_ref[t, :, :hid] = block[:half, :]
        out_ref[t, :, hid:] = block[half:, :]


def partial_body(own_ref, tiles_ref, weights_ref, out_ref):
    peers, rows, _ = out_ref.shape
    width = weights_ref.shape[1]
    step = rows // CHUNKS
    length = step * width // LANES
    own = own_ref[0]
    for i in range(CHUNKS):
        block = tiles_ref[pl.ds(i * length, length), :].astype(F32)
        block = block.reshape(step, width).astype(BF16)
        for t in range(peers):
            target = lax.rem(own - t + peers, peers)
            out_ref[target, pl.ds(i * step, step), :] = jnp.dot(
                block, weights_ref[t], preferred_element_type=F32
            ).astype(BF16)


def hidden_body(sums_ref, out_ref):
    peers, _, hid = out_ref.shape
    total = sums_ref[0].astype(F32)
    for q in range(1, peers):
        total = total + sums_ref[q].astype(F32)
    gate, up = total[:, :hid], total[:, hid:]
    hidden = (gate / (1.0 + jnp.exp(-gate)) * up).astype(BF16)
    for q in range(peers):
        out_ref[q] = hidden


def down_body(hidden_ref, weights_ref, out_ref):
    peers, rows, _ = hidden_ref.shape
    width = weights_ref.shape[1]
    step = rows // 3
    for i in range(3):
        at = pl.ds(i * step, step)
        hidden = jnp.concatenate([hidden_ref[q, at, :] for q in range(peers)], axis=1)
        result = jnp.dot(hidden, weights_ref[...], preferred_element_type=F32)
        tiles = width // LANES
        out_ref[pl.ds(i * step * tiles, step * tiles), :] = result.reshape(
            step * tiles, LANES
        ).astype(BF16)


def lend_body(tiles_ref, pick_ref, lent_ref, rows_ref):
    rows, width = rows_ref.shape
    step = rows // CHUNKS
    length = step * width // LANES
    for i in range(CHUNKS):
        block = tiles_ref[pl.ds(i * length, length), :].astype(F32)
        rows_ref[pl.ds(i * step, step), :] = block.reshape(step, width).astype(BF16)
    both = jnp.concatenate([pick_ref[1, k] for k in range(TOP_K)], axis=0)
    lent = jnp.dot(both, rows_ref[...], preferred_element_type=F32).astype(BF16)
    lent_ref[...] = lent.reshape(lent_ref.shape)


def keep_body(rows_ref, pick_ref, share_ref, tokens_ref, mixed_ref):
    mixed = residual_scale * tokens_ref[...].astype(F32)
    for k in range(TOP_K):
        kept = jnp.dot(pick_ref[0, k], rows_ref[...], preferred_element_type=F32)
        mixed = mixed + share_ref[k][:, 0:1] * kept
    mixed_ref[...] = mixed


def mix_body(part_ref, other_ref, share_ref, mixed_ref, sums_ref):
    mixed = part_ref[...]
    for k in range(TOP_K):
        mixed = mixed + share_ref[k][:, 0:1] * other_ref[k].astype(F32)
    count = mixed.shape[0]
    mixed_ref[...] = mixed
    first = jnp.sum(mixed, axis=1, keepdims=True)
    second = jnp.sum(mixed * mixed, axis=1, keepdims=True)
    lane = lax.broadcasted_iota(jnp.int32, (count, count), 1)
    both = jnp.where(lane == 0, first, jnp.where(lane == 1, second, 0.0)).T[:8, :]
    for q in range(sums_ref.shape[0]):
        sums_ref[q] = both


def norm_body(mixed_ref, sums_ref, gain_ref, bias_ref, out_ref):
    total = sums_ref[0]
    for q in range(1, sums_ref.shape[0]):
        total = total + sums_ref[q]
    center = total[0:1, :] / D
    spread = total[1:2, :] / D - center * center
    scale = lax.rsqrt(spread + norm_eps)
    count = out_ref.shape[0]
    center = jnp.broadcast_to(center, (count, count)).T[:, 0:1]
    scale = jnp.broadcast_to(scale, (count, count)).T[:, 0:1]
    normed = (mixed_ref[...] - center) * scale * gain_ref[...] + bias_ref[...]
    out_ref[...] = normed.astype(BF16)


def on_device(
    tokens, expert_ids, group_weight, expert_weight, w_gate, w_up, w_down, norm_gain, norm_bias
):
    tok_count, width = tokens.shape
    expert_count = lax.axis_size(EP)
    peers = lax.axis_size("tp")
    hid = w_gate.shape[2]
    capacity = min(tok_count // GROUPS, 3 * TOP_K * tok_count // (2 * expert_count))
    rows = expert_count * capacity
    tiles = rows * width // LANES
    chips = expert_count // CORES
    ids = expert_ids.T
    own = lax.axis_index("tp").astype(jnp.int32).reshape(1)
    core = lax.axis_index("ep_2").astype(jnp.int32).reshape(1)
    smem = pl.BlockSpec(memory_space=pltpu.SMEM)
    swap = [(c, CORES - 1 - c) for c in range(CORES)]
    hbm = pl.BlockSpec(memory_space=pl.ANY)
    bundle = pl.pallas_call(
        bundle_body,
        in_specs=[hbm] * 2,
        out_specs=in_vmem(1)[0],
        out_shape=jax.ShapeDtypeStruct((tok_count + 8, width), BF16),
        scratch_shapes=[pltpu.VMEM(ids.shape, ids.dtype), pltpu.SemaphoreType.DMA((2,))],
        compiler_params=pltpu.CompilerParams(vmem_limit_bytes=2 << 20),
        name="bundle",
    )(ids, tokens)
    peer = lax.ppermute(bundle, "ep_2", swap)

    outgoing, peer_ids = pl.pallas_call(
        functools.partial(send_body, capacity=capacity, lag=LAG),
        in_specs=[smem, hbm, hbm, hbm],
        out_specs=[hbm, hbm],
        out_shape=(
            jax.ShapeDtypeStruct((tiles, LANES), BF16),
            jax.ShapeDtypeStruct(ids.shape, ids.dtype),
        ),
        scratch_shapes=[
            pltpu.VMEM(ids.shape, ids.dtype),
            pltpu.VMEM(ids.shape, ids.dtype),
            pltpu.VMEM((8, tok_count), BF16),
            pltpu.VMEM((CORES * tok_count, width), tokens.dtype),
            pltpu.VMEM((CHUNKS, tiles // CHUNKS, LANES), BF16),
            pltpu.SemaphoreType.DMA((2 * CORES + CHUNKS + 1,)),
        ],
        compiler_params=pltpu.CompilerParams(vmem_limit_bytes=6 << 20),
        name="send",
    )(core, ids, bundle, peer)
    def weights_of(w_gate, w_up):
        both = [w.reshape(peers, width, hid) for w in (w_gate, w_up)]
        return permuted(jnp.concatenate(both, axis=1), "tp")

    def packed_of(blocks):
        return pl.pallas_call(
            pack_body,
            in_specs=[smem, *in_vmem(peers)],
            out_specs=in_vmem(1)[0],
            out_shape=jax.ShapeDtypeStruct((peers, width, 2 * hid), BF16),
            compiler_params=pltpu.CompilerParams(vmem_limit_bytes=6 << 20),
            name="pack",
        )(own, *blocks)

    def picked(peer_ids):
        return pl.pallas_call(
            functools.partial(pick_body, capacity=capacity),
            in_specs=[smem, *in_vmem(4)],
            out_specs=in_vmem(2),
            out_shape=(
                jax.ShapeDtypeStruct((CORES, TOP_K, tok_count, rows), BF16),
                jax.ShapeDtypeStruct((TOP_K, tok_count, tok_count), F32),
            ),
            compiler_params=pltpu.CompilerParams(vmem_limit_bytes=3 << 20),
            name="pick",
        )(core, ids, peer_ids, group_weight[None, :], expert_weight.T)

    def partial_of(arrived, blocks, peer_ids):
        packed, pick, share = lax.optimization_barrier((packed_of(blocks), *picked(peer_ids)))
        partial = pl.pallas_call(
            partial_body,
            in_specs=[smem, *in_vmem(2)],
            out_specs=in_vmem(1)[0],
            out_shape=jax.ShapeDtypeStruct((peers, rows, 2 * hid), BF16),
            compiler_params=pltpu.CompilerParams(vmem_limit_bytes=6 << 20),
            name="partial",
        )(own, arrived.reshape(tiles, LANES), packed)
        return partial, pick, share

    def rows_first(outgoing, peer_ids, w_gate, w_up):
        arrived = exchanged(outgoing, CHIPS)
        return partial_of(arrived, weights_of(w_gate, w_up), peer_ids)

    def weights_first(outgoing, peer_ids, w_gate, w_up):
        blocks = weights_of(w_gate, w_up)
        held = [blocks[t] for t in HELD]
        outgoing = pl.pallas_call(
            hold_body,
            in_specs=[pl.BlockSpec(memory_space=pl.ANY)] * (1 + len(held)),
            out_specs=pl.BlockSpec(memory_space=pl.ANY),
            out_shape=jax.ShapeDtypeStruct(outgoing.shape, outgoing.dtype),
            input_output_aliases={0: 0},
            compiler_params=pltpu.CompilerParams(vmem_limit_bytes=1 << 20),
            name="hold",
        )(outgoing, *held)
        return partial_of(exchanged(outgoing, CHIPS), blocks, peer_ids)

    partial, pick, share = lax.cond(
        core[0] == LATE,
        weights_first,
        rows_first,
        outgoing.reshape(chips, tiles // chips, LANES),
        peer_ids,
        w_gate,
        w_up,
    )
    summed = exchanged(partial, "tp")
    hidden = pl.pallas_call(
        hidden_body,
        in_specs=in_vmem(1),
        out_specs=in_vmem(1)[0],
        out_shape=jax.ShapeDtypeStruct((peers, rows, hid), BF16),
        compiler_params=pltpu.CompilerParams(vmem_limit_bytes=3 << 20),
        name="hidden",
    )(summed)
    hidden = exchanged(hidden, "tp")
    result = pl.pallas_call(
        down_body,
        in_specs=in_vmem(2),
        out_specs=in_vmem(1)[0],
        out_shape=jax.ShapeDtypeStruct((tiles, LANES), BF16),
        compiler_params=pltpu.CompilerParams(vmem_limit_bytes=4 << 20),
        name="down",
    )(hidden, w_down[0])
    returned = exchanged(result.reshape(chips, tiles // chips, LANES), CHIPS)
    lent, kept_rows = pl.pallas_call(
        lend_body,
        in_specs=in_vmem(2),
        out_specs=in_vmem(2),
        out_shape=(
            jax.ShapeDtypeStruct((TOP_K, tok_count, width), BF16),
            jax.ShapeDtypeStruct((rows, width), BF16),
        ),
        compiler_params=pltpu.CompilerParams(vmem_limit_bytes=4 << 20),
        name="lend",
    )(returned.reshape(tiles, LANES), pick)
    other = lax.ppermute(lent, "ep_2", swap)
    part = pl.pallas_call(
        keep_body,
        in_specs=in_vmem(4),
        out_specs=in_vmem(1)[0],
        out_shape=jax.ShapeDtypeStruct((tok_count, width), F32),
        compiler_params=pltpu.CompilerParams(vmem_limit_bytes=4 << 20),
        name="keep",
    )(kept_rows, pick, share, tokens)
    mixed, sums = pl.pallas_call(
        mix_body,
        in_specs=in_vmem(3),
        out_specs=in_vmem(2),
        out_shape=(
            jax.ShapeDtypeStruct((tok_count, width), F32),
            jax.ShapeDtypeStruct((peers, 8, tok_count), F32),
        ),
        compiler_params=pltpu.CompilerParams(vmem_limit_bytes=4 << 20),
        name="mix",
    )(part, other, share)
    sums = exchanged(sums, "tp")
    return pl.pallas_call(
        norm_body,
        out_shape=jax.ShapeDtypeStruct((tok_count, width), BF16),
        compiler_params=pltpu.CompilerParams(vmem_limit_bytes=2 << 20),
        name="norm",
    )(mixed, sums, norm_gain[None, :], norm_bias[None, :])


def solution(mesh):
    finer = Mesh(mesh.devices.reshape(16, 4, 2, mesh.shape["tp"]), ("ep_0", "ep_1", "ep_2", "tp"))
    placed = (
        P(EP, "tp"),
        P(EP, None),
        P(EP),
        P(EP, None),
        P(EP, None, "tp"),
        P(EP, None, "tp"),
        P(EP, None, "tp"),
        P("tp"),
        P("tp"),
    )
    return jax.shard_map(
        on_device, mesh=finer, in_specs=placed, out_specs=P(EP, "tp"), check_vma=False
    )
```

```python
import functools

import jax
import jax.numpy as jnp
from jax import lax
from jax.experimental import pallas as pl
from jax.experimental.pallas import tpu as pltpu
from jax.sharding import Mesh
from jax.sharding import PartitionSpec as P

D = 4096
GROUPS = 4
TOP_K = 2
EP = ("ep_0", "ep_1", "ep_2")
CHIPS = ("ep_0", "ep_1")
CORES = 2
LAG = 0
LATE = 1
HELD = (1, 2, 3)
LANES = 128
CHUNKS = 3
PIECES = 2
F32 = jnp.float32
BF16 = jnp.bfloat16


residual_scale = 2.0**0.5
norm_eps = 1e-05


def exchanged(tiles, axis):
    return lax.all_to_all(tiles, axis, 0, 0, tiled=True)


def in_vmem(count):
    return [pl.BlockSpec(memory_space=pltpu.VMEM) for _ in range(count)]


def permuted(tiles, axis):
    peers = lax.axis_size(axis)
    own = lax.axis_index(axis)
    result = [lax.dynamic_index_in_dim(tiles, own, 0, keepdims=False)]
    for turn in range(1, peers):
        block = lax.dynamic_index_in_dim(tiles, (own + turn) % peers, 0, keepdims=False)
        moves = [(i, (i + turn) % peers) for i in range(peers)]
        result.append(lax.ppermute(block, axis, moves))
    return result


def positions(ids, capacity, core, block):
    count = ids.shape[1]
    rows = [jnp.broadcast_to(ids[k : k + 1, :], (count, count)) for k in range(TOP_K)]
    columns = [r.T for r in rows]
    earlier = lax.broadcasted_iota(jnp.int32, (count, count), 0) < lax.broadcasted_iota(
        jnp.int32, (count, count), 1
    )
    found = []
    for k in range(TOP_K):
        same = sum(
            (jnp.where((c == rows[k]) & earlier, 1.0, 0.0) for c in columns),
            jnp.zeros((count, count), F32),
        )
        before = jnp.sum(same, axis=0, keepdims=True)
        for j in range(k):
            before = before + jnp.where(ids[j : j + 1, :] == ids[k : k + 1, :], 1.0, 0.0)
        chosen = ids[k : k + 1, :]
        chip = lax.shift_right_logical(chosen, 1)
        row = (chip * CORES + block) * capacity + before.astype(jnp.int32)
        found.append(jnp.where((chosen & 1) == core, row, -1))
    return found


def bundle_body(ids_hbm, tokens_hbm, out_ref, ids_ref, sems):
    count = tokens_hbm.shape[0]
    fetch_ids = pltpu.make_async_copy(ids_hbm, ids_ref, sems.at[0])
    fetch_tokens = pltpu.make_async_copy(tokens_hbm, out_ref.at[pl.ds(0, count)], sems.at[1])
    fetch_ids.start()
    fetch_tokens.start()
    extra = out_ref.shape[0] - count
    fetch_ids.wait()
    line = lax.broadcasted_iota(jnp.int32, (extra, count), 0)
    marks = jnp.where(line == 0, ids_ref[0:1, :], ids_ref[1:2, :])
    out_ref[count:, :count] = marks.astype(F32).astype(BF16)
    fetch_tokens.wait()


def hold_body(rows_hbm, *refs):
    del rows_hbm, refs


def send_body(
    core_ref,
    ids_hbm,
    own_hbm,
    peer_hbm,
    out_hbm,
    peer_ids_out,
    ids_ref,
    peer_ids_ref,
    marks_ref,
    tokens_ref,
    out_ref,
    sems,
    *,
    capacity,
    lag,
):
    chunks, length, _ = out_ref.shape
    extra, count = marks_ref.shape
    width = own_hbm.shape[1]
    fetch_ids = [
        pltpu.make_async_copy(ids_hbm, ids_ref, sems.at[0]),
        pltpu.make_async_copy(
            peer_hbm.at[pl.ds(count, extra), pl.ds(0, count)], marks_ref, sems.at[1]
        ),
    ]
    fetch_tokens = [
        pltpu.make_async_copy(
            t.at[pl.ds(0, count)], tokens_ref.at[pl.ds(b * count, count)], sems.at[CORES + b]
        )
        for b, t in enumerate((own_hbm, peer_hbm))
    ]
    for f in fetch_ids + fetch_tokens:
        f.start()
    core = core_ref[0]
    step = length * LANES // width
    slots = lax.broadcasted_iota(jnp.int32, (step, count), 0)
    for f in fetch_ids:
        f.wait()
    peer_ids_ref[...] = marks_ref[...].astype(F32).astype(jnp.int32)[0:TOP_K, :]
    save_ids = pltpu.make_async_copy(peer_ids_ref, peer_ids_out, sems.at[2 * CORES + chunks])
    save_ids.start()
    where = [
        positions(ids[...], capacity, core, b) for b, ids in enumerate((ids_ref, peer_ids_ref))
    ]
    select = []
    for i in range(chunks):
        marks = [
            jnp.where((slots == w[0] - i * step) | (slots == w[1] - i * step), 1.0, 0.0)
            for w in where
        ]
        select.append(jnp.concatenate(marks, axis=1).astype(BF16))
    for f in fetch_tokens:
        f.wait()
    stores = []
    for i in range(chunks):
        outgoing = jnp.dot(select[i], tokens_ref[...], preferred_element_type=F32)
        out_ref[i] = outgoing.reshape(length, LANES).astype(BF16)
        store = pltpu.make_async_copy(
            out_ref.at[i], out_hbm.at[pl.ds(i * length, length)], sems.at[2 * CORES + i]
        )
        store.start()
        stores.append(store)
    for store in stores + [save_ids]:
        store.wait()

    if lag:

        @pl.when(core == LATE)
        def _():
            pl.delay(lag)


def pick_body(core_ref, ids_ref, peer_ids_ref, group_ref, weight_ref, pick_ref, share_ref, *, capacity):
    rows = pick_ref.shape[3]
    count = ids_ref.shape[1]
    core = core_ref[0]
    slots = lax.broadcasted_iota(jnp.int32, (rows, count), 0)
    for b, ids in enumerate((ids_ref, peer_ids_ref)):
        where = positions(ids[...], capacity, core, b)
        for k in range(TOP_K):
            pick_ref[b, k] = jnp.where(slots == where[k], 1.0, 0.0).T.astype(BF16)
    weight = weight_ref[...]
    total = weight[0:1, :] + weight[1:2, :]
    for k in range(TOP_K):
        share = group_ref[...] * weight[k : k + 1, :] / total
        share_ref[k] = jnp.broadcast_to(share, (count, count)).T


def pack_body(own_ref, *refs):
    out_ref = refs[-1]
    half = out_ref.shape[1]
    hid = out_ref.shape[2] // 2
    for t, block in enumerate(refs[:-1]):
        out_ref[t, :, :hid] = block[:half, :]
        out_ref[t, :, hid:] = block[half:, :]


def partial_body(own_ref, tiles_ref, weights_ref, out_ref):
    peers, rows, _ = out_ref.shape
    width = weights_ref.shape[1]
    step = rows // PIECES
    length = step * width // LANES
    own = own_ref[0]
    for i in range(PIECES):
        block = tiles_ref[pl.ds(i * length, length), :].astype(F32)
        block = block.reshape(step, width).astype(BF16)
        for t in range(peers):
            target = lax.rem(own - t + peers, peers)
            out_ref[target, pl.ds(i * step, step), :] = jnp.dot(
                block, weights_ref[t], preferred_element_type=F32
            ).astype(BF16)


def hidden_body(sums_ref, out_ref):
    peers, _, hid = out_ref.shape
    total = sums_ref[0].astype(F32)
    for q in range(1, peers):
        total = total + sums_ref[q].astype(F32)
    gate, up = total[:, :hid], total[:, hid:]
    hidden = (gate / (1.0 + jnp.exp(-gate)) * up).astype(BF16)
    for q in range(peers):
        out_ref[q] = hidden


def down_body(hidden_ref, weights_ref, out_ref):
    peers, rows, _ = hidden_ref.shape
    width = weights_ref.shape[1]
    step = rows // 3
    for i in range(3):
        at = pl.ds(i * step, step)
        hidden = jnp.concatenate([hidden_ref[q, at, :] for q in range(peers)], axis=1)
        result = jnp.dot(hidden, weights_ref[...], preferred_element_type=F32)
        tiles = width // LANES
        out_ref[pl.ds(i * step * tiles, step * tiles), :] = result.reshape(
            step * tiles, LANES
        ).astype(BF16)


def lend_body(tiles_ref, pick_ref, lent_ref, rows_ref):
    rows, width = rows_ref.shape
    step = rows // CHUNKS
    length = step * width // LANES
    for i in range(CHUNKS):
        block = tiles_ref[pl.ds(i * length, length), :].astype(F32)
        rows_ref[pl.ds(i * step, step), :] = block.reshape(step, width).astype(BF16)
    both = jnp.concatenate([pick_ref[1, k] for k in range(TOP_K)], axis=0)
    lent = jnp.dot(both, rows_ref[...], preferred_element_type=F32).astype(BF16)
    lent_ref[...] = lent.reshape(lent_ref.shape)


def keep_body(rows_ref, pick_ref, share_ref, tokens_ref, mixed_ref):
    mixed = residual_scale * tokens_ref[...].astype(F32)
    for k in range(TOP_K):
        kept = jnp.dot(pick_ref[0, k], rows_ref[...], preferred_element_type=F32)
        mixed = mixed + share_ref[k][:, 0:1] * kept
    mixed_ref[...] = mixed


def mix_body(part_ref, other_ref, share_ref, mixed_ref, sums_ref):
    mixed = part_ref[...]
    for k in range(TOP_K):
        mixed = mixed + share_ref[k][:, 0:1] * other_ref[k].astype(F32)
    count = mixed.shape[0]
    mixed_ref[...] = mixed
    first = jnp.sum(mixed, axis=1, keepdims=True)
    second = jnp.sum(mixed * mixed, axis=1, keepdims=True)
    lane = lax.broadcasted_iota(jnp.int32, (count, count), 1)
    both = jnp.where(lane == 0, first, jnp.where(lane == 1, second, 0.0)).T[:8, :]
    for q in range(sums_ref.shape[0]):
        sums_ref[q] = both


def norm_body(mixed_ref, sums_ref, gain_ref, bias_ref, out_ref):
    total = sums_ref[0]
    for q in range(1, sums_ref.shape[0]):
        total = total + sums_ref[q]
    center = total[0:1, :] / D
    spread = total[1:2, :] / D - center * center
    scale = lax.rsqrt(spread + norm_eps)
    count = out_ref.shape[0]
    center = jnp.broadcast_to(center, (count, count)).T[:, 0:1]
    scale = jnp.broadcast_to(scale, (count, count)).T[:, 0:1]
    normed = (mixed_ref[...] - center) * scale * gain_ref[...] + bias_ref[...]
    out_ref[...] = normed.astype(BF16)


def on_device(
    tokens, expert_ids, group_weight, expert_weight, w_gate, w_up, w_down, norm_gain, norm_bias
):
    tok_count, width = tokens.shape
    expert_count = lax.axis_size(EP)
    peers = lax.axis_size("tp")
    hid = w_gate.shape[2]
    capacity = min(tok_count // GROUPS, 3 * TOP_K * tok_count // (2 * expert_count))
    rows = expert_count * capacity
    tiles = rows * width // LANES
    chips = expert_count // CORES
    ids = expert_ids.T
    own = lax.axis_index("tp").astype(jnp.int32).reshape(1)
    core = lax.axis_index("ep_2").astype(jnp.int32).reshape(1)
    smem = pl.BlockSpec(memory_space=pltpu.SMEM)
    swap = [(c, CORES - 1 - c) for c in range(CORES)]
    hbm = pl.BlockSpec(memory_space=pl.ANY)
    bundle = pl.pallas_call(
        bundle_body,
        in_specs=[hbm] * 2,
        out_specs=in_vmem(1)[0],
        out_shape=jax.ShapeDtypeStruct((tok_count + 8, width), BF16),
        scratch_shapes=[pltpu.VMEM(ids.shape, ids.dtype), pltpu.SemaphoreType.DMA((2,))],
        compiler_params=pltpu.CompilerParams(vmem_limit_bytes=2 << 20),
        name="bundle",
    )(ids, tokens)
    peer = lax.ppermute(bundle, "ep_2", swap)

    outgoing, peer_ids = pl.pallas_call(
        functools.partial(send_body, capacity=capacity, lag=LAG),
        in_specs=[smem, hbm, hbm, hbm],
        out_specs=[hbm, hbm],
        out_shape=(
            jax.ShapeDtypeStruct((tiles, LANES), BF16),
            jax.ShapeDtypeStruct(ids.shape, ids.dtype),
        ),
        scratch_shapes=[
            pltpu.VMEM(ids.shape, ids.dtype),
            pltpu.VMEM(ids.shape, ids.dtype),
            pltpu.VMEM((8, tok_count), BF16),
            pltpu.VMEM((CORES * tok_count, width), tokens.dtype),
            pltpu.VMEM((CHUNKS, tiles // CHUNKS, LANES), BF16),
            pltpu.SemaphoreType.DMA((2 * CORES + CHUNKS + 1,)),
        ],
        compiler_params=pltpu.CompilerParams(vmem_limit_bytes=6 << 20),
        name="send",
    )(core, ids, bundle, peer)
    def weights_of(w_gate, w_up):
        both = [w.reshape(peers, width, hid) for w in (w_gate, w_up)]
        return permuted(jnp.concatenate(both, axis=1), "tp")

    def packed_of(blocks):
        return pl.pallas_call(
            pack_body,
            in_specs=[smem, *in_vmem(peers)],
            out_specs=in_vmem(1)[0],
            out_shape=jax.ShapeDtypeStruct((peers, width, 2 * hid), BF16),
            compiler_params=pltpu.CompilerParams(vmem_limit_bytes=6 << 20),
            name="pack",
        )(own, *blocks)

    def picked(peer_ids):
        return pl.pallas_call(
            functools.partial(pick_body, capacity=capacity),
            in_specs=[smem, *in_vmem(4)],
            out_specs=in_vmem(2),
            out_shape=(
                jax.ShapeDtypeStruct((CORES, TOP_K, tok_count, rows), BF16),
                jax.ShapeDtypeStruct((TOP_K, tok_count, tok_count), F32),
            ),
            compiler_params=pltpu.CompilerParams(vmem_limit_bytes=3 << 20),
            name="pick",
        )(core, ids, peer_ids, group_weight[None, :], expert_weight.T)

    def partial_of(arrived, blocks, peer_ids):
        packed, pick, share = lax.optimization_barrier((packed_of(blocks), *picked(peer_ids)))
        partial = pl.pallas_call(
            partial_body,
            in_specs=[smem, *in_vmem(2)],
            out_specs=in_vmem(1)[0],
            out_shape=jax.ShapeDtypeStruct((peers, rows, 2 * hid), BF16),
            compiler_params=pltpu.CompilerParams(vmem_limit_bytes=6 << 20),
            name="partial",
        )(own, arrived.reshape(tiles, LANES), packed)
        return partial, pick, share

    def rows_first(outgoing, peer_ids, w_gate, w_up):
        arrived = exchanged(outgoing, CHIPS)
        return partial_of(arrived, weights_of(w_gate, w_up), peer_ids)

    def weights_first(outgoing, peer_ids, w_gate, w_up):
        blocks = weights_of(w_gate, w_up)
        held = [blocks[t] for t in HELD]
        outgoing = pl.pallas_call(
            hold_body,
            in_specs=[pl.BlockSpec(memory_space=pl.ANY)] * (1 + len(held)),
            out_specs=pl.BlockSpec(memory_space=pl.ANY),
            out_shape=jax.ShapeDtypeStruct(outgoing.shape, outgoing.dtype),
            input_output_aliases={0: 0},
            compiler_params=pltpu.CompilerParams(vmem_limit_bytes=1 << 20),
            name="hold",
        )(outgoing, *held)
        return partial_of(exchanged(outgoing, CHIPS), blocks, peer_ids)

    partial, pick, share = lax.cond(
        core[0] == LATE,
        weights_first,
        rows_first,
        outgoing.reshape(chips, tiles // chips, LANES),
        peer_ids,
        w_gate,
        w_up,
    )
    summed = exchanged(partial, "tp")
    hidden = pl.pallas_call(
        hidden_body,
        in_specs=in_vmem(1),
        out_specs=in_vmem(1)[0],
        out_shape=jax.ShapeDtypeStruct((peers, rows, hid), BF16),
        compiler_params=pltpu.CompilerParams(vmem_limit_bytes=3 << 20),
        name="hidden",
    )(summed)
    hidden = exchanged(hidden, "tp")
    result = pl.pallas_call(
        down_body,
        in_specs=in_vmem(2),
        out_specs=in_vmem(1)[0],
        out_shape=jax.ShapeDtypeStruct((tiles, LANES), BF16),
        compiler_params=pltpu.CompilerParams(vmem_limit_bytes=4 << 20),
        name="down",
    )(hidden, w_down[0])
    returned = exchanged(result.reshape(chips, tiles // chips, LANES), CHIPS)
    lent, kept_rows = pl.pallas_call(
        lend_body,
        in_specs=in_vmem(2),
        out_specs=in_vmem(2),
        out_shape=(
            jax.ShapeDtypeStruct((TOP_K, tok_count, width), BF16),
            jax.ShapeDtypeStruct((rows, width), BF16),
        ),
        compiler_params=pltpu.CompilerParams(vmem_limit_bytes=4 << 20),
        name="lend",
    )(returned.reshape(tiles, LANES), pick)
    other = lax.ppermute(lent, "ep_2", swap)
    part = pl.pallas_call(
        keep_body,
        in_specs=in_vmem(4),
        out_specs=in_vmem(1)[0],
        out_shape=jax.ShapeDtypeStruct((tok_count, width), F32),
        compiler_params=pltpu.CompilerParams(vmem_limit_bytes=4 << 20),
        name="keep",
    )(kept_rows, pick, share, tokens)
    mixed, sums = pl.pallas_call(
        mix_body,
        in_specs=in_vmem(3),
        out_specs=in_vmem(2),
        out_shape=(
            jax.ShapeDtypeStruct((tok_count, width), F32),
            jax.ShapeDtypeStruct((peers, 8, tok_count), F32),
        ),
        compiler_params=pltpu.CompilerParams(vmem_limit_bytes=4 << 20),
        name="mix",
    )(part, other, share)
    sums = exchanged(sums, "tp")
    return pl.pallas_call(
        norm_body,
        out_shape=jax.ShapeDtypeStruct((tok_count, width), BF16),
        compiler_params=pltpu.CompilerParams(vmem_limit_bytes=2 << 20),
        name="norm",
    )(mixed, sums, norm_gain[None, :], norm_bias[None, :])


def solution(mesh):
    finer = Mesh(mesh.devices.reshape(16, 4, 2, mesh.shape["tp"]), ("ep_0", "ep_1", "ep_2", "tp"))
    placed = (
        P(EP, "tp"),
        P(EP, None),
        P(EP),
        P(EP, None),
        P(EP, None, "tp"),
        P(EP, None, "tp"),
        P(EP, None, "tp"),
        P("tp"),
        P("tp"),
    )
    return jax.shard_map(
        on_device, mesh=finer, in_specs=placed, out_specs=P(EP, "tp"), check_vma=False
    )
```
